256 devices in a mesh: ep: 128 (over z, y, x), tp: 2 (over core).
Axes of the slice: x: 4, y: 4, z: 8, core: 2. Of those that a mesh axis runs over, the one named last changes fastest.
Arguments:
- tokens: bfloat16 [3072, 2048], P('ep'), may hold values from -40 to 40
- old_state: float32 [3072, 16, 4096], P('ep', 'tp'), may hold values from -6 to 6
- w_query: bfloat16 [2048, 1024], P(None, 'tp'), may hold values from -0.125 to 0.125
- w_forget: bfloat16 [2048, 1024], P(None, 'tp'), may hold values from -0.125 to 0.125
- w_value: bfloat16 [2048, 1024], P(None, 'tp'), may hold values from -0.125 to 0.125
- w_gate: bfloat16 [2048, 1024], P(None, 'tp'), may hold values from -0.125 to 0.125
- lower_bound: float32 [1024], P('tp'), may hold values from 0.05 to 0.9
- head_gain: float32 [64], replicated, may hold values from 0.1 to 1.9
- w_out: bfloat16 [1024, 2048], P('tp'), may hold values from -0.1875 to 0.1875
- mix_gain: float32 [2048], replicated, may hold values from 0.1 to 1.9
- expert_gate: bfloat16 [128, 2048, 512], P('ep', None, 'tp'), may hold values from -0.125 to 0.125
- expert_up: bfloat16 [128, 2048, 512], P('ep', None, 'tp'), may hold values from -0.125 to 0.125
- expert_down: bfloat16 [128, 512, 2048], P('ep', 'tp'), may hold values from -0.25 to 0.25
- expert_ids: int32 [3072, 2], P('ep'), may hold values from 0 to 127, as said below
- route_weight: float32 [3072, 2], P('ep'), may hold values from 0.1 to 1
- moe_gain: float32 [2048], replicated, may hold values from 0.1 to 1.9
Outputs:
- next_tokens: bfloat16 [3072, 2048], P('ep', 'tp')
- new_state: float32 [3072, 16, 4096], P('ep', 'tp')
The draws below stay inside these ranges and needn't reach their ends.
Inputs may be any that keep to these rules, and one draw needn't show every extreme that they name: `expert_ids`: each row names two different experts of one group of 4 consecutive experts. In each aligned block of 24 rows no expert is named by more than 2 rows, and one expert, the same in every block, is named by exactly 2 rows of every block.
All inputs are finite; a program needn't handle non-finite values.
Results may differ from the reference program's by a relative error of at most 0.011.
Values may be sent and summed in bfloat16 or wider, within the bound.
A program may use at most 128 MiB of HBM per device.

```python
import math
import jax
import jax.numpy as jnp
from jax import lax

D = 2048
HEADS = 16
HD = 64
FF = 512
EPG = 4
TOPK = 2
SEQ_DEV = 24
HW = 1024
SEQS = 3072
EXPERTS = 128
GROUPS = 32
CAP = 2
N_TP = 2


def draw_tokens(key, part):
    draw_keys = jax.random.split(key, 4)
    column_scale = jnp.exp(jax.random.uniform(draw_keys[0], (D,), jnp.float32, 0.0, math.log(10.0)))
    column_scale = column_scale / jnp.sqrt(jnp.mean(column_scale * column_scale))
    row_scale = jnp.exp(jax.random.uniform(draw_keys[1], (SEQS, 1), jnp.float32, math.log(0.5), math.log(2.0)))
    noise = jax.random.normal(draw_keys[3], (SEQS, D), jnp.float32)
    noise = jnp.clip(noise, -6.0, 6.0)
    return (noise * column_scale[None, :] * row_scale).astype(jnp.bfloat16)


def draw_expert_ids(key, part):
    block_count = SEQS // SEQ_DEV
    lane_count = GROUPS * 2 * CAP
    popular = jax.random.randint(jax.random.fold_in(key, 1), (GROUPS,), 1, 9)
    forced_group = jax.random.randint(jax.random.fold_in(key, 2), (), 0, GROUPS)
    base_scores = jax.random.randint(jax.random.fold_in(key, 3), (EPG,), 0, 1024) * EPG + jnp.arange(EPG)
    base_order = jnp.argsort(base_scores, stable=True)

    def one_block(block_key):
        block_keys = jax.random.split(block_key, 3)
        order_scores = jax.random.randint(block_keys[0], (GROUPS, EPG), 0, 1024) * EPG + jnp.arange(EPG)[None, :]
        orders = jnp.argsort(order_scores, axis=1, stable=True)
        orders = jnp.where((jnp.arange(GROUPS) == forced_group)[:, None], base_order[None, :], orders)
        lane_ids = jnp.arange(lane_count)
        lane_group = lane_ids // (2 * CAP)
        lane_pair = lane_ids % (2 * CAP) // CAP
        lane_score = jax.random.randint(block_keys[1], (lane_count,), 0, 16384) * popular[lane_group]
        forced = (lane_group == forced_group) & (lane_pair == 0)
        lane_rank = lane_score * 4096 + lane_ids + jnp.where(forced, 1 << 30, 0)
        chosen = lax.top_k(lane_rank.astype(jnp.int32), SEQ_DEV)[1]
        chosen = jax.random.permutation(block_keys[2], chosen)
        row_group = lane_group[chosen]
        row_pair = lane_pair[chosen]
        first_expert = orders[row_group, 2 * row_pair] + row_group * EPG
        second_expert = orders[row_group, 2 * row_pair + 1] + row_group * EPG
        return jnp.stack([first_expert, second_expert], 1)
    routed = jax.vmap(one_block)(jax.random.split(jax.random.fold_in(key, 4), block_count))
    return routed.reshape(SEQS, TOPK).astype(jnp.int32)


def level_of(stream_key, dims, cuts, least, high):
    def one(axis_at, shards_of):
        draws = jax.random.uniform(jax.random.fold_in(jax.random.fold_in(stream_key, 6), axis_at), (shards_of,), jnp.float32, least / len(cuts), high / len(cuts))
        return jnp.repeat(jnp.exp(draws), dims[axis_at] // shards_of).reshape((-1,) + (1,) * (len(dims) - axis_at - 1))

    level = one(*cuts[0])
    for cut in cuts[1:]:
        level = level * one(*cut)
    return level


def normal_values(key, extent, spread, most, cuts=(), held_as=jnp.bfloat16):
    factor_of = level_of(key, extent, cuts, -0.22, 0.18) if cuts else 1.0
    array = jax.random.normal(key, extent, jnp.float32) * spread * factor_of
    return jnp.minimum(jnp.maximum(array, -most), most).astype(held_as)


def setup_inputs(seed: int = 0) -> dict:
    arg_keys = jax.random.split(jax.random.key(seed), 17)
    return {
        "tokens": draw_tokens(jax.random.fold_in(arg_keys[16], 71), 0),
        "old_state": normal_values(arg_keys[1], (SEQS, HEADS, HD * HD), 1.0, 6.0, ((0, 128), (1, 2)), jnp.float32),
        "w_query": normal_values(arg_keys[2], (D, HW), D ** -0.5, 0.125, ((1, 2),)),
        "w_forget": normal_values(arg_keys[3], (D, HW), D ** -0.5, 0.125, ((1, 2),)),
        "w_value": normal_values(arg_keys[4], (D, HW), D ** -0.5, 0.125, ((1, 2),)),
        "w_gate": normal_values(arg_keys[5], (D, HW), D ** -0.5, 0.125, ((1, 2),)),
        "lower_bound": jnp.clip(0.05 + 0.84999998 * jax.random.uniform(arg_keys[6], (HW,), jnp.float32) ** level_of(arg_keys[6], (HW,), ((0, 2),), -0.2, 0.2), 0.05, 0.9),
        "head_gain": jnp.clip(1.0 + 0.18 * jax.random.normal(arg_keys[7], (HD,), jnp.float32), 0.1, 1.9),
        "w_out": normal_values(arg_keys[8], (HW, D), HW ** -0.5, 0.1875, ((0, 2),)),
        "mix_gain": jnp.clip(1.0 + 0.18 * jax.random.normal(arg_keys[9], (D,), jnp.float32), 0.1, 1.9),
        "expert_gate": normal_values(arg_keys[10], (EXPERTS, D, FF), D ** -0.5, 0.125, ((0, 128), (2, 2))),
        "expert_up": normal_values(arg_keys[11], (EXPERTS, D, FF), D ** -0.5, 0.125, ((0, 128), (2, 2))),
        "expert_down": normal_values(arg_keys[12], (EXPERTS, FF, D), FF ** -0.5, 0.25, ((0, 128), (1, 2))),
        "expert_ids": draw_expert_ids(jax.random.fold_in(arg_keys[16], 71), 0),
        "route_weight": jnp.clip(jnp.exp(math.log(1.0) - 2.3025851 * jax.random.uniform(arg_keys[14], (SEQS, TOPK), jnp.float32) ** level_of(arg_keys[14], (SEQS, TOPK), ((0, 128),), -0.2, 0.2)), 0.1, 1.0),
        "moe_gain": jnp.clip(1.0 + 0.18 * jax.random.normal(arg_keys[15], (D,), jnp.float32), 0.1, 1.9),
    }


def layer_normed(values, gain):
    center = lax.optimization_barrier(jnp.mean(values, -1, keepdims=True))
    centered = values - center
    variance = lax.optimization_barrier(jnp.mean(centered * centered, -1, keepdims=True))
    return centered * lax.rsqrt(variance + 1e-05) * gain

def rounded(values):
    return lax.optimization_barrier(values.astype(jnp.bfloat16)).astype(jnp.float32)

def slot_table(ids_block, expert_count, capacity):
    flat_ids = ids_block.reshape(-1)
    onehot = (flat_ids[:, None] == jnp.arange(expert_count, dtype=jnp.int32)[None, :]).astype(jnp.int32)
    before = jnp.cumsum(onehot, 0) - onehot
    rank = lax.optimization_barrier(jnp.sum(before * onehot, 1)).astype(jnp.int32)
    return (flat_ids * capacity + rank).astype(jnp.int32)

def reference(tokens, old_state, w_query, w_forget, w_value, w_gate, lower_bound, head_gain, w_out, mix_gain, expert_gate, expert_up, expert_down, expert_ids, route_weight, moe_gain):
    row_count = tokens.shape[0]
    half_cols = HW // N_TP
    q_lin = jnp.dot(tokens, w_query, preferred_element_type=jnp.float32)
    f_lin = jnp.dot(tokens, w_forget, preferred_element_type=jnp.float32)
    v_lin = jnp.dot(tokens, w_value, preferred_element_type=jnp.float32)
    g_lin = jnp.dot(tokens, w_gate, preferred_element_type=jnp.float32)
    act_query = jax.nn.silu(q_lin).reshape(row_count, HEADS, HD)
    bound = lower_bound.reshape(HEADS, HD)
    forget = bound + (1.0 - bound) * jax.nn.sigmoid(f_lin.reshape(row_count, HEADS, HD))
    previous = old_state.reshape(row_count, HEADS, HD, HD)
    new_state = forget[..., None] * previous + (1.0 - forget)[..., None] * v_lin.reshape(row_count, HEADS, 1, HD)
    readout = jnp.einsum('shi,shij->shj', act_query, new_state, precision=lax.Precision.HIGHEST)
    normed = readout * lax.rsqrt(lax.optimization_barrier(jnp.mean(readout * readout, -1, keepdims=True)) + 1e-06) * head_gain
    mixer_out = (normed * jax.nn.silu(g_lin.reshape(row_count, HEADS, HD))).reshape(row_count, HW).astype(jnp.bfloat16)
    mixed = jnp.zeros((row_count, D), jnp.float32)
    for half_index in range(N_TP):
        lower = half_index * half_cols
        mixed = mixed + rounded(jnp.dot(mixer_out[:, lower:lower + half_cols], w_out[lower:lower + half_cols], preferred_element_type=jnp.float32))
    after_mixer = layer_normed(tokens.astype(jnp.float32) + mixed, mix_gain).astype(jnp.bfloat16)
    block_count = row_count // SEQ_DEV
    slot_count = EXPERTS * CAP
    id_blocks = expert_ids.reshape(block_count, SEQ_DEV, TOPK)
    slot_ids = jax.vmap(lambda one_block: slot_table(one_block, EXPERTS, CAP))(id_blocks)
    placing = (slot_ids[:, None, :] == jnp.arange(slot_count, dtype=jnp.int32)[None, :, None]).astype(jnp.float32)
    choose = placing.reshape(block_count, slot_count, SEQ_DEV, TOPK).sum(-1)
    row_blocks = after_mixer.reshape(block_count, SEQ_DEV, D).astype(jnp.float32)
    buffer = jnp.einsum('bcs,bsd->bcd', choose, row_blocks, precision=lax.Precision.HIGHEST).astype(jnp.bfloat16)
    by_expert = buffer.reshape(block_count, EXPERTS, CAP, D).transpose(1, 0, 2, 3).reshape(EXPERTS, block_count * CAP, D)
    half_units = FF // N_TP

    def run_expert(inputs):
        rows_in, gate_weight, up_weight, down_weight = inputs
        gate_act = jnp.dot(rows_in, gate_weight, preferred_element_type=jnp.float32)
        up_act = jnp.dot(rows_in, up_weight, preferred_element_type=jnp.float32)
        hidden = (jax.nn.silu(gate_act) * up_act).astype(jnp.bfloat16)
        total = jnp.zeros((rows_in.shape[0], D), jnp.float32)
        for half_index in range(N_TP):
            lower = half_index * half_units
            total = total + rounded(jnp.dot(hidden[:, lower:lower + half_units], down_weight[lower:lower + half_units], preferred_element_type=jnp.float32))
        return total.astype(jnp.bfloat16)
    results = lax.map(run_expert, (by_expert, expert_gate, expert_up, expert_down))
    returned = results.reshape(EXPERTS, block_count, CAP, D).transpose(1, 0, 2, 3).reshape(block_count, slot_count, D)
    picked = jnp.take_along_axis(returned, slot_ids[:, :, None], axis=1)
    picked = picked.reshape(row_count, TOPK, D).astype(jnp.float32)
    moe_sum = lax.optimization_barrier(jnp.sum(picked * route_weight[..., None], 1))
    next_tokens = layer_normed(after_mixer.astype(jnp.float32) + moe_sum, moe_gain).astype(jnp.bfloat16)
    return (next_tokens, new_state.reshape(row_count, HEADS, HD * HD))
```

```python
import functools

import jax
import jax.numpy as jnp
from jax import lax
from jax.experimental import pallas as pl
from jax.experimental.pallas import tpu as pltpu
from jax.sharding import PartitionSpec as P

MESH = pl.DeviceIdType.MESH
BF = jnp.bfloat16
F32 = jnp.float32


def dot(a, b):
    return jnp.dot(a, b, preferred_element_type=F32)


def silu(v):
    return v / (1.0 + jnp.exp(-v))


def kernel(
    n_ep,
    tokens,
    old,
    w_query,
    w_forget,
    w_value,
    w_gate,
    bound,
    head_gain,
    w_out,
    mix_gain,
    e_gate,
    e_up,
    e_down,
    ids,
    weight,
    moe_gain,
    next_out,
    state_out,
    tok,
    wq,
    wf,
    wv,
    wg,
    st,
    wo,
    eg,
    eu,
    ed,
    f_s,
    q_s,
    v_s,
    r_s,
    mix,
    own_part,
    other_part,
    after,
    send,
    recv_a,
    recv_b,
    down_send,
    down_recv,
    ret_send,
    ret_recv,
    stat_send,
    stat_recv,
    in_sem,
    out_sem,
    tp_send,
    tp_recv,
    ep_send,
    ep_recv,
):
    me = lax.axis_index("ep")
    core = lax.axis_index("tp")
    rows, width = tok.shape
    heads = st.shape[1]
    half = width // 2
    blocks = half // 128
    own_cols = pl.multiple_of(core * half, 128)
    other_cols = pl.multiple_of((1 - core) * half, 128)
    n_slots = 2 * n_ep

    seqs = rows // 3
    loads = [
        pltpu.make_async_copy(src, dst, in_sem.at[i])
        for i, (src, dst) in enumerate(
            (
                (tokens, tok),
                (w_forget, wf),
                (w_value, wv),
                (w_query, wq),
                (old.at[pl.ds(0, seqs)], st.at[pl.ds(0, seqs)]),
                (old.at[pl.ds(seqs, seqs)], st.at[pl.ds(seqs, seqs)]),
                (old.at[pl.ds(2 * seqs, seqs)], st.at[pl.ds(2 * seqs, seqs)]),
                (w_gate, wg),
                (w_out, wo),
                (e_gate.at[0], eg),
                (e_up.at[0], eu),
                (e_down.at[0], ed),
            )
        )
    ]
    for load in loads:
        load.start()

    barrier = pltpu.get_barrier_semaphore()
    pl.semaphore_signal(barrier, inc=1, device_id=(me, 1 - core), device_id_type=MESH)

    def greet(i, carry):
        peer = lax.rem(me + i, n_ep)
        pl.semaphore_signal(barrier, inc=1, device_id=(peer, core), device_id_type=MESH)
        return carry

    lax.fori_loop(1, n_ep, greet, 0)

    slot_iota = lax.broadcasted_iota(jnp.int32, (rows, n_slots), 1)
    expert_iota = lax.shift_right_logical(slot_iota, 1)
    id0 = ids[:, 0:1]
    id1 = ids[:, 1:2]
    names0 = expert_iota == id0
    names1 = expert_iota == id1
    named = jnp.where(names0 | names1, 1.0, 0.0)
    r_iota = lax.broadcasted_iota(jnp.int32, (rows, rows), 0)
    c_iota = lax.broadcasted_iota(jnp.int32, (rows, rows), 1)
    earlier = jnp.where(c_iota < r_iota, 1.0, 0.0)
    rank = dot(earlier.astype(BF), named.astype(BF))
    slot_of = lax.bitwise_and(slot_iota, 1).astype(F32)
    takes = jnp.where(rank == slot_of, named, 0.0)
    route = jnp.where(names0, weight[:, 0:1], 0.0) + jnp.where(names1, weight[:, 1:2], 0.0)
    route = jnp.where(rank == slot_of, route, 0.0)
    route_high = route.astype(BF)
    route_low = (route - route_high.astype(F32)).astype(BF)
    choose = takes.T.astype(BF)

    pairs = heads // 2

    def by_head(ref, values, p):
        ref[pl.ds(2 * p, rows, heads), :] = values
        ref[pl.ds(2 * p + 1, rows, heads), :] = values

    loads[0].wait()
    x = tok[...]
    loads[1].wait()
    f_lin = dot(x, wf[...])
    for p in range(pairs):
        cols = slice(p * 128, (p + 1) * 128)
        low = bound[:, cols]
        by_head(f_s, low + (1.0 - low) / (1.0 + jnp.exp(-f_lin[:, cols])), p)
    loads[2].wait()
    v_lin = dot(x, wv[...])
    for p in range(pairs):
        by_head(v_s, v_lin[:, p * 128 : (p + 1) * 128], p)
    loads[3].wait()
    q_lin = dot(x, wq[...])
    for p in range(pairs):
        by_head(q_s, silu(q_lin[:, p * 128 : (p + 1) * 128]), p)

    lane = lax.broadcasted_iota(jnp.int32, (heads, 128), 1)
    head = lax.broadcasted_iota(jnp.int32, (heads, 128), 0)
    odd = lax.bitwise_and(head, 1) * 64
    key_at = odd + lax.shift_right_logical(lane, 6)
    value_at = odd + lax.bitwise_and(lane, 63)
    n_cols = st.shape[2] // 128

    def one_sequence(s, carry):
        at = pl.ds(pl.multiple_of(s * heads, heads), heads)
        f_row = f_s[at, :]
        q_row = q_s[at, :]
        v_row = jnp.take_along_axis(v_s[at, :], value_at, axis=1)
        sums = [jnp.zeros((heads, 128), F32) for _ in range(4)]
        for c in range(n_cols):
            key = key_at + 2 * c
            f_here = jnp.take_along_axis(f_row, key, axis=1)
            q_here = jnp.take_along_axis(q_row, key, axis=1)
            new = v_row + f_here * (st[s, :, c * 128 : (c + 1) * 128] - v_row)
            st[s, :, c * 128 : (c + 1) * 128] = new
            sums[c % 4] = sums[c % 4] + q_here * new
        total = (sums[0] + sums[1]) + (sums[2] + sums[3])
        r_s[at, :] = total + pltpu.roll(total, 64, 1)
        return carry

    outs = []
    for part in range(3):
        loads[4 + part].wait()
        lax.fori_loop(part * seqs, (part + 1) * seqs, one_sequence, 0)
        out = pltpu.make_async_copy(
            st.at[pl.ds(part * seqs, seqs)],
            state_out.at[pl.ds(part * seqs, seqs)],
            out_sem.at[part],
        )
        out.start()
        outs.append(out)

    loads[7].wait()
    g_lin = dot(x, wg[...])
    first_head = lax.broadcasted_iota(jnp.int32, (rows, 128), 1) < 64
    gain2 = jnp.concatenate([head_gain[...], head_gain[...]], axis=1)
    for p in range(pairs):
        cols = slice(p * 128, (p + 1) * 128)
        even_head = r_s[pl.ds(2 * p, rows, heads), :]
        odd_head = r_s[pl.ds(2 * p + 1, rows, heads), :]
        even_head = even_head * lax.rsqrt(
            jnp.sum(even_head * even_head, -1, keepdims=True) / 128.0 + 1e-6
        )
        odd_head = odd_head * lax.rsqrt(
            jnp.sum(odd_head * odd_head, -1, keepdims=True) / 128.0 + 1e-6
        )
        normed = jnp.where(first_head, even_head, odd_head) * gain2
        mix[:, cols] = (normed * silu(g_lin[:, cols])).astype(BF)
    loads[8].wait()
    own_part[...] = dot(mix[...], wo[...]).astype(BF)

    pl.semaphore_wait(barrier, n_ep)

    def to_partner(src, dst, i):
        return pltpu.make_async_remote_copy(
            src_ref=src,
            dst_ref=dst,
            send_sem=tp_send.at[i],
            recv_sem=tp_recv.at[i],
            device_id=(me, 1 - core),
            device_id_type=MESH,
        )

    swap = to_partner(own_part, other_part, 0)
    swap.start()
    swap.wait()
    mixed = own_part[...].astype(F32) + other_part[...].astype(F32)
    full = x.astype(F32) + mixed
    centered = full - jnp.mean(full, -1, keepdims=True)
    variance = jnp.mean(centered * centered, -1, keepdims=True)
    after[...] = (centered * lax.rsqrt(variance + 1e-5) * mix_gain[...]).astype(BF)

    after_half = after[:, pl.ds(own_cols, half)]
    for j in range(blocks):
        picked = dot(choose, after_half[:, j * 128 : (j + 1) * 128]).astype(BF)
        send[j] = picked.reshape(n_ep, 2, 128)

    def exchange(src, dst, i):
        def one(k, carry):
            peer = lax.rem(me + k, n_ep)
            pltpu.make_async_remote_copy(
                src_ref=src.at[:, peer],
                dst_ref=dst.at[:, me],
                send_sem=ep_send.at[i],
                recv_sem=ep_recv.at[i],
                device_id=(peer, core),
                device_id_type=MESH,
            ).start()
            return carry

        lax.fori_loop(1, n_ep, one, 0)
        dst[:, pl.ds(me, 1)] = src[:, pl.ds(me, 1)]

    def exchanged(src, dst, i):
        whole = pltpu.make_async_remote_copy(
            src_ref=src.at[:, pl.ds(0, n_ep - 1)],
            dst_ref=dst.at[:, pl.ds(0, n_ep - 1)],
            send_sem=ep_send.at[i],
            recv_sem=ep_recv.at[i],
            device_id=(me, 1 - core),
            device_id_type=MESH,
        )
        return whole

    exchange(send, recv_a, 0)
    dispatched = exchanged(send, recv_a, 0)
    dispatched.wait_recv()
    forward = to_partner(recv_a, recv_b, 1)
    forward.start()
    for i in (9, 10, 11):
        loads[i].wait()

    def project(buf, weights, first):
        total = jnp.zeros((n_slots, weights.shape[1]), F32)
        for j in range(blocks):
            total += dot(
                buf[j].reshape(n_slots, 128),
                weights[pl.ds(pl.multiple_of(first + j * 128, 128), 128), :],
            )
        return total

    gate_act = project(recv_a, eg, own_cols)
    up_act = project(recv_a, eu, own_cols)
    forward.wait_recv()
    gate_act += project(recv_b, eg, other_cols)
    up_act += project(recv_b, eu, other_cols)
    hidden = (silu(gate_act) * up_act).astype(BF)

    down_send[...] = dot(hidden, ed[:, pl.ds(other_cols, half)]).astype(BF)
    meet = to_partner(down_send, down_recv, 2)
    meet.start()
    kept = dot(hidden, ed[:, pl.ds(own_cols, half)]).astype(BF).astype(F32)
    meet.wait_recv()
    summed = (kept + down_recv[...].astype(F32)).astype(BF)
    for j in range(blocks):
        ret_send[j] = summed[:, j * 128 : (j + 1) * 128].reshape(n_ep, 2, 128)
    exchange(ret_send, ret_recv, 1)
    returned = exchanged(ret_send, ret_recv, 1)
    returned.wait_recv()

    route_both = jnp.concatenate([route_high.astype(F32), route_low.astype(F32)], axis=0).astype(BF)
    sums = []
    for j in range(blocks):
        both = dot(route_both, ret_recv[j].reshape(n_slots, 128))
        sums.append(both[:rows] + both[rows:])
    moe_sum = jnp.concatenate(sums, axis=1)
    final = after[:, pl.ds(own_cols, half)].astype(F32) + moe_sum
    own_mean = jnp.mean(final, -1, keepdims=True)
    off = final - own_mean
    own_var = jnp.mean(off * off, -1, keepdims=True)
    stat_send[...] = jnp.where(first_head, own_mean, own_var)
    stats = to_partner(stat_send, stat_recv, 3)
    stats.start()
    stats.wait_recv()
    other_mean = stat_recv[:, 0:1]
    other_var = stat_recv[:, 64:65]
    gap = own_mean - other_mean
    mean = 0.5 * (own_mean + other_mean)
    variance = 0.5 * (own_var + other_var) + 0.25 * gap * gap
    gain = moe_gain[:, pl.ds(own_cols, half)]
    next_out[...] = ((final - mean) * lax.rsqrt(variance + 1e-5) * gain).astype(BF)

    for out in outs:
        out.wait()
    dispatched.wait_send()
    returned.wait_send()
    for remote in (forward, meet, stats):
        remote.wait_send()


def per_device(
    tokens,
    old_state,
    w_query,
    w_forget,
    w_value,
    w_gate,
    lower_bound,
    head_gain,
    w_out,
    mix_gain,
    expert_gate,
    expert_up,
    expert_down,
    expert_ids,
    route_weight,
    moe_gain,
):
    n_ep = lax.axis_size("ep")
    rows, width = tokens.shape
    heads = old_state.shape[1]
    cols = w_query.shape[1]
    units = expert_gate.shape[2]
    half = width // 2
    blocks = half // 128
    n_slots = 2 * n_ep
    anywhere = pl.BlockSpec(memory_space=pl.ANY)
    vmem = pl.BlockSpec(memory_space=pltpu.VMEM)
    message = pltpu.VMEM((blocks, n_ep, 2, 128), BF)
    return pl.pallas_call(
        functools.partial(kernel, n_ep),
        out_shape=(
            jax.ShapeDtypeStruct((rows, half), BF),
            jax.ShapeDtypeStruct(old_state.shape, F32),
        ),
        in_specs=[
            anywhere,
            anywhere,
            anywhere,
            anywhere,
            anywhere,
            anywhere,
            vmem,
            vmem,
            anywhere,
            vmem,
            anywhere,
            anywhere,
            anywhere,
            vmem,
            vmem,
            vmem,
        ],
        out_specs=(vmem, anywhere),
        scratch_shapes=[
            pltpu.VMEM((rows, width), BF),
            pltpu.VMEM((width, cols), BF),
            pltpu.VMEM((width, cols), BF),
            pltpu.VMEM((width, cols), BF),
            pltpu.VMEM((width, cols), BF),
            pltpu.VMEM(old_state.shape, F32),
            pltpu.VMEM((cols, width), BF),
            pltpu.VMEM((width, units), BF),
            pltpu.VMEM((width, units), BF),
            pltpu.VMEM((units, width), BF),
            pltpu.VMEM((rows * heads, 128), F32),
            pltpu.VMEM((rows * heads, 128), F32),
            pltpu.VMEM((rows * heads, 128), F32),
            pltpu.VMEM((rows * heads, 128), F32),
            pltpu.VMEM((rows, cols), BF),
            pltpu.VMEM((rows, width), BF),
            pltpu.VMEM((rows, width), BF),
            pltpu.VMEM((rows, width), BF),
            message,
            message,
            message,
            pltpu.VMEM((n_slots, half), BF),
            pltpu.VMEM((n_slots, half), BF),
            message,
            message,
            pltpu.VMEM((rows, 128), F32),
            pltpu.VMEM((rows, 128), F32),
            pltpu.SemaphoreType.DMA((12,)),
            pltpu.SemaphoreType.DMA((3,)),
            pltpu.SemaphoreType.DMA((4,)),
            pltpu.SemaphoreType.DMA((4,)),
            pltpu.SemaphoreType.DMA((2,)),
            pltpu.SemaphoreType.DMA((2,)),
        ],
        compiler_params=pltpu.CompilerParams(
            collective_id=0, has_side_effects=True, vmem_limit_bytes=56 * 1024 * 1024
        ),
    )(
        tokens,
        old_state,
        w_query,
        w_forget,
        w_value,
        w_gate,
        lower_bound.reshape(1, cols),
        head_gain.reshape(1, -1),
        w_out,
        mix_gain.reshape(1, width),
        expert_gate,
        expert_up,
        expert_down,
        expert_ids,
        route_weight,
        moe_gain.reshape(1, width),
    )


def solution(mesh):
    in_specs = (
        P("ep", None),
        P("ep", "tp", None),
        P(None, "tp"),
        P(None, "tp"),
        P(None, "tp"),
        P(None, "tp"),
        P("tp"),
        P(),
        P("tp", None),
        P(),
        P("ep", None, "tp"),
        P("ep", None, "tp"),
        P("ep", "tp", None),
        P("ep", None),
        P("ep", None),
        P(),
    )
    out_specs = (P("ep", "tp"), P("ep", "tp", None))
    return jax.shard_map(
        per_device, mesh=mesh, in_specs=in_specs, out_specs=out_specs, check_vma=False
    )
```

```python
import jax
import jax.numpy as jnp
from jax import lax
from jax.experimental import pallas as pl
from jax.experimental.pallas import tpu as pltpu
from jax.sharding import PartitionSpec as P

MESH = pl.DeviceIdType.MESH
BF = jnp.bfloat16
F32 = jnp.float32


def dot(a, b):
    return jnp.dot(a, b, preferred_element_type=F32)


def silu(v):
    return v / (1.0 + jnp.exp(-v))


AXES = (8, 4, 4)
PLANE = AXES[1] * AXES[2]
Z_ORDER = (4, 3, 5, 2, 6, 1, 7, 0)
GROUPS = ((0, 1), (1, 3), (3, 5), (5, 8))
SELF = 7 * PLANE


def kernel(
    tokens,
    old,
    w_query,
    w_forget,
    w_value,
    w_gate,
    bound_in,
    head_gain_in,
    w_out,
    mix_gain_in,
    e_gate,
    e_up,
    e_down,
    ids_in,
    weight_in,
    moe_gain_in,
    next_out,
    st,
    tok,
    wq,
    wf,
    wv,
    wg,
    wo,
    eg,
    eu,
    ed,
    bound,
    head_gain,
    mix_gain,
    ids,
    weight,
    moe_gain,
    f_s,
    q_s,
    v_s,
    r_s,
    gates,
    mix,
    own_part,
    other_part,
    after,
    send,
    recv_a,
    recv_b,
    down_keep,
    down_send,
    down_recv,
    ret_send,
    ret_recv,
    stat_send,
    stat_recv,
    small,
    in_sem,
    tp_send,
    tp_recv,
    ep_send,
    ep_recv,
):
    me = lax.axis_index("ep")
    core = lax.axis_index("tp")
    n_ep = AXES[0] * PLANE
    rows, width = tok.shape
    heads = st.shape[1]
    half = width // 2
    blocks = half // 128
    own_cols = pl.multiple_of(core * half, 128)
    other_cols = pl.multiple_of((1 - core) * half, 128)
    n_slots = 2 * n_ep
    n_keys = st.shape[2]
    my_z = lax.div(me, PLANE)
    my_y = lax.rem(lax.div(me, AXES[2]), AXES[1])
    my_x = lax.rem(me, AXES[2])

    def at_offset(dz, r, sign):
        dy = lax.div(r, AXES[2])
        dx = lax.rem(r, AXES[2])
        if sign < 0:
            dz, dy, dx = AXES[0] - dz, AXES[1] - dy, AXES[2] - dx
        return (
            lax.rem(my_z + dz, AXES[0]) * PLANE
            + lax.rem(my_y + dy, AXES[1]) * AXES[2]
            + lax.rem(my_x + dx, AXES[2])
        )

    part = n_keys // 4
    pieces = [
        (tokens, tok),
        (bound_in, bound),
        (w_forget, wf),
        (w_query, wq),
        (w_value, wv),
        *((old.at[:, :, pl.ds(i * part, part)], st.at[:, :, pl.ds(i * part, part)]) for i in range(4)),
        (w_gate, wg),
        (head_gain_in, head_gain),
        (w_out, wo),
        (mix_gain_in, mix_gain),
        (ids_in, ids),
        (weight_in, weight),
        (e_gate.at[0], eg),
        (e_up.at[0], eu),
        (e_down.at[0], ed),
        (moe_gain_in, moe_gain),
    ]
    loads = [pltpu.make_async_copy(src, dst, in_sem.at[i]) for i, (src, dst) in enumerate(pieces)]
    for load in loads:
        load.start()
    l_tok, l_bound, l_wf, l_wq, l_wv = loads[:5]
    l_state = loads[5:9]
    l_wg, l_hg, l_wo, l_mg, l_ids, l_weight, l_eg, l_eu, l_ed, l_og = loads[9:]

    barrier = pltpu.get_barrier_semaphore()
    pl.semaphore_signal(barrier, inc=1, device_id=(me, 1 - core), device_id_type=MESH)
    for pos, dz in enumerate(Z_ORDER):

        def greet(r, carry, dz=dz):
            peer = at_offset(dz, r, 1)
            pl.semaphore_signal(barrier, inc=1, device_id=(peer, core), device_id_type=MESH)
            return carry

        lax.fori_loop(1 if dz == 0 else 0, PLANE, greet, 0)

    pairs = heads // 2
    tall = rows * heads

    def by_head(ref, values, p):
        ref[pl.ds(2 * p, rows, heads), :] = values
        ref[pl.ds(2 * p + 1, rows, heads), :] = values

    lane = lax.broadcasted_iota(jnp.int32, (tall, 128), 1)
    head = lax.broadcasted_iota(jnp.int32, (tall, 128), 0)
    mine = lax.shift_right_logical(lane, 6) == lax.bitwise_and(head, 1)

    def split(ref, first):
        values = jnp.where(mine, ref[...], 0.0)
        high = values.astype(BF)
        gates[first : first + tall, 0:128] = high
        gates[first : first + tall, 128:256] = (values - high.astype(F32)).astype(BF)

    l_tok.wait()
    x = tok[...]
    l_bound.wait()
    l_wf.wait()
    f_lin = dot(x, wf[...])
    for p in range(pairs):
        cols = slice(p * 128, (p + 1) * 128)
        low = bound[:, cols]
        by_head(f_s, low + (1.0 - low) / (1.0 + jnp.exp(-f_lin[:, cols])), p)
    split(f_s, 0)
    l_wq.wait()
    q_lin = dot(x, wq[...])
    for p in range(pairs):
        by_head(q_s, silu(q_lin[:, p * 128 : (p + 1) * 128]), p)
    split(q_s, tall)
    l_wv.wait()
    v_lin = dot(x, wv[...])
    for p in range(pairs):
        by_head(v_s, v_lin[:, p * 128 : (p + 1) * 128], p)
    v_pair = v_s[...]
    v_s[...] = jnp.where(mine, v_pair, pltpu.roll(v_pair, 64, 1))
    r_s[...] = jnp.zeros_like(r_s)

    tile = 256
    key_gap = (
        lax.bitwise_and(lax.broadcasted_iota(jnp.int32, (tile, tile), 0), 63)
        - lax.shift_right_logical(lax.broadcasted_iota(jnp.int32, (tile, tile), 1), 6)
    ).astype(F32)

    def one_tile(n, carry):
        spread = jnp.where(key_gap == (4 * n).astype(F32), 1.0, 0.0).astype(BF)
        both = dot(gates[...], spread)
        cols = pl.ds(pl.multiple_of(n * tile, tile), tile)
        previous = st[:, :, cols].reshape(tall, tile)
        value = jnp.concatenate([v_s[...], v_s[...]], axis=1)
        new = value + both[:tall] * (previous - value)
        st[:, :, cols] = new.reshape(rows, heads, tile)
        read = both[tall:] * new
        r_s[...] += read[:, :128] + read[:, 128:]
        return carry

    per_part = part // tile
    for i in range(4):
        l_state[i].wait()
        lax.fori_loop(i * per_part, (i + 1) * per_part, one_tile, 0)
    r_s[...] += pltpu.roll(r_s[...], 64, 1)

    l_wg.wait()
    l_hg.wait()
    g_lin = dot(x, wg[...])
    first_head = lax.broadcasted_iota(jnp.int32, (rows, 128), 1) < 64
    gain2 = jnp.concatenate([head_gain[...], head_gain[...]], axis=1)
    for p in range(pairs):
        cols = slice(p * 128, (p + 1) * 128)
        even_head = r_s[pl.ds(2 * p, rows, heads), :]
        odd_head = r_s[pl.ds(2 * p + 1, rows, heads), :]
        even_head = even_head * lax.rsqrt(
            jnp.sum(even_head * even_head, -1, keepdims=True) / 128.0 + 1e-6
        )
        odd_head = odd_head * lax.rsqrt(
            jnp.sum(odd_head * odd_head, -1, keepdims=True) / 128.0 + 1e-6
        )
        normed = jnp.where(first_head, even_head, odd_head) * gain2
        mix[:, cols] = (normed * silu(g_lin[:, cols])).astype(BF)
    l_wo.wait()
    own_part[...] = dot(mix[...], wo[...]).astype(BF)

    pl.semaphore_wait(barrier, n_ep)

    def to_partner(src, dst, i):
        return pltpu.make_async_remote_copy(
            src_ref=src,
            dst_ref=dst,
            send_sem=tp_send.at[i],
            recv_sem=tp_recv.at[i],
            device_id=(me, 1 - core),
            device_id_type=MESH,
        )

    swap = to_partner(own_part, other_part, 0)
    swap.start()

    for load in (l_ids, l_weight, l_mg):
        load.wait()
    small[...] = jnp.zeros_like(small)
    small[0:2, 0:rows] = ids[...].astype(F32)
    small[2:4, 0:rows] = weight[...]
    turned = small[...].T[0:rows]
    id0 = turned[:, 0:1].astype(jnp.int32)
    id1 = turned[:, 1:2].astype(jnp.int32)
    slot_iota = lax.broadcasted_iota(jnp.int32, (rows, n_slots), 1)
    slot_pos = lax.shift_right_logical(slot_iota, 5)
    dz = jnp.zeros_like(slot_pos)
    for pos, offset in enumerate(Z_ORDER):
        dz = jnp.where(slot_pos == pos, offset, dz)
    dy = lax.bitwise_and(lax.shift_right_logical(slot_iota, 3), 3)
    dx = lax.bitwise_and(lax.shift_right_logical(slot_iota, 1), 3)
    expert = (
        lax.bitwise_and(my_z + dz, 7) * PLANE
        + lax.bitwise_and(my_y + dy, 3) * AXES[2]
        + lax.bitwise_and(my_x + dx, 3)
    )
    names0 = expert == id0
    names1 = expert == id1
    named = jnp.where(names0 | names1, 1.0, 0.0)
    r_iota = lax.broadcasted_iota(jnp.int32, (rows, rows), 0)
    c_iota = lax.broadcasted_iota(jnp.int32, (rows, rows), 1)
    earlier = jnp.where(c_iota < r_iota, 1.0, 0.0)
    rank = dot(earlier.astype(BF), named.astype(BF))
    slot_of = lax.bitwise_and(slot_iota, 1).astype(F32)
    takes = jnp.where(rank == slot_of, named, 0.0)
    route = jnp.where(names0, turned[:, 2:3], 0.0) + jnp.where(names1, turned[:, 3:4], 0.0)
    route = jnp.where(rank == slot_of, route, 0.0)
    route_high = route.astype(BF)
    route_low = (route - route_high.astype(F32)).astype(BF)
    route_both = jnp.concatenate([route_high.astype(F32), route_low.astype(F32)], axis=0).astype(BF)
    choose = takes.T.astype(BF)
    swap.wait()
    mixed = own_part[...].astype(F32) + other_part[...].astype(F32)
    full = x.astype(F32) + mixed
    centered = full - jnp.mean(full, -1, keepdims=True)
    variance = jnp.mean(centered * centered, -1, keepdims=True)
    after[...] = (centered * lax.rsqrt(variance + 1e-5) * mix_gain[...]).astype(BF)

    def exchange(src, dst, send_sem, recv_sem, group, sign):
        for pos in range(*group):

            def one(r, carry, pos=pos):
                k = pos * PLANE + r
                pltpu.make_async_remote_copy(
                    src_ref=src.at[:, k],
                    dst_ref=dst.at[:, k],
                    send_sem=send_sem,
                    recv_sem=recv_sem,
                    device_id=(at_offset(Z_ORDER[pos], r, sign), core),
                    device_id_type=MESH,
                ).start()
                return carry

            lax.fori_loop(1 if pos == 7 else 0, PLANE, one, 0)
        if group[1] == 8:
            dst[:, SELF : SELF + 1] = src[:, SELF : SELF + 1]

    def bytes_of(src, dst, send_sem, recv_sem, first, count):
        return pltpu.make_async_remote_copy(
            src_ref=src.at[:, pl.ds(first, count)],
            dst_ref=dst.at[:, pl.ds(first, count)],
            send_sem=send_sem,
            recv_sem=recv_sem,
            device_id=(me, 1 - core),
            device_id_type=MESH,
        )

    def arrived(src, dst, send_sem, recv_sem, group):
        first, last = group[0] * PLANE, group[1] * PLANE
        count = last - first - (1 if group[1] == 8 else 0)
        bytes_of(src, dst, send_sem, recv_sem, first, count).wait_recv()

    after_half = after[:, pl.ds(own_cols, half)]
    for g, group in enumerate(GROUPS):
        first, last = group[0] * PLANE, group[1] * PLANE
        picked = dot(choose[2 * first : 2 * last], after_half).astype(BF)
        for j in range(blocks):
            send[j, first:last] = picked[:, j * 128 : (j + 1) * 128].reshape(last - first, 2, 128)
        exchange(send, recv_a, ep_send.at[0], ep_recv.at[g], group, 1)

    for load in (l_eg, l_eu, l_ed, l_og):
        load.wait()

    def project(buf, weights, first_row, first, last):
        total = None
        for j in range(blocks):
            term = dot(
                buf[j, first:last].reshape(2 * (last - first), 128),
                weights[pl.ds(pl.multiple_of(first_row + j * 128, 128), 128), :],
            )
            total = term if total is None else total + term
        return total

    forwards = []
    meets = []

    def arrive(g):
        group = GROUPS[g]
        first, last = group[0] * PLANE, group[1] * PLANE
        arrived(send, recv_a, ep_send.at[0], ep_recv.at[g], group)
        forward = to_partner(recv_a.at[:, pl.ds(first, last - first)], recv_b.at[:, pl.ds(first, last - first)], 2 + g)
        forward.start()
        forwards.append(forward)

    def compute(g):
        group = GROUPS[g]
        first, last = group[0] * PLANE, group[1] * PLANE
        at = slice(2 * first, 2 * last)
        gate_act = project(recv_a, eg, own_cols, first, last)
        up_act = project(recv_a, eu, own_cols, first, last)
        forwards[g].wait_recv()
        gate_act += project(recv_b, eg, other_cols, first, last)
        up_act += project(recv_b, eu, other_cols, first, last)
        hidden = (silu(gate_act) * up_act).astype(BF)
        down_send[at] = dot(hidden, ed[:, pl.ds(other_cols, half)]).astype(BF)
        meet = to_partner(
            down_send.at[pl.ds(2 * first, 2 * (last - first))],
            down_recv.at[pl.ds(2 * first, 2 * (last - first))],
            6 + g,
        )
        meet.start()
        meets.append(meet)
        down_keep[at] = dot(hidden, ed[:, pl.ds(own_cols, half)]).astype(BF)

    def give_back(g):
        group = GROUPS[g]
        first, last = group[0] * PLANE, group[1] * PLANE
        at = slice(2 * first, 2 * last)
        meets[g].wait_recv()
        summed = (down_keep[at].astype(F32) + down_recv[at].astype(F32)).astype(BF)
        for j in range(blocks):
            ret_send[j, first:last] = summed[:, j * 128 : (j + 1) * 128].reshape(last - first, 2, 128)
        exchange(ret_send, ret_recv, ep_send.at[1], ep_recv.at[4 + g], group, -1)

    for g in range(len(GROUPS)):
        arrive(g)
        if g > 0:
            give_back(g - 1)
        compute(g)
    give_back(len(GROUPS) - 1)

    moe_sum = None
    for g, group in enumerate(GROUPS):
        first, last = group[0] * PLANE, group[1] * PLANE
        arrived(ret_send, ret_recv, ep_send.at[1], ep_recv.at[4 + g], group)
        sums = []
        for j in range(blocks):
            sums.append(
                dot(
                    route_both[:, 2 * first : 2 * last],
                    ret_recv[j, first:last].reshape(2 * (last - first), 128),
                )
            )
        both = jnp.concatenate(sums, axis=1)
        both = both[:rows] + both[rows:]
        moe_sum = both if moe_sum is None else moe_sum + both
    final = after[:, pl.ds(own_cols, half)].astype(F32) + moe_sum
    own_mean = jnp.mean(final, -1, keepdims=True)
    off = final - own_mean
    own_var = jnp.mean(off * off, -1, keepdims=True)
    stat_send[...] = jnp.where(first_head, own_mean, own_var)
    stats = to_partner(stat_send, stat_recv, 1)
    stats.start()
    stats.wait_recv()
    other_mean = stat_recv[:, 0:1]
    other_var = stat_recv[:, 64:65]
    gap = own_mean - other_mean
    mean = 0.5 * (own_mean + other_mean)
    variance = 0.5 * (own_var + other_var) + 0.25 * gap * gap
    gain = moe_gain[:, pl.ds(own_cols, half)]
    next_out[...] = ((final - mean) * lax.rsqrt(variance + 1e-5) * gain).astype(BF)

    bytes_of(send, recv_a, ep_send.at[0], ep_recv.at[0], 0, n_ep - 1).wait_send()
    bytes_of(ret_send, ret_recv, ep_send.at[1], ep_recv.at[4], 0, n_ep - 1).wait_send()
    for remote in (*forwards, *meets, stats):
        remote.wait_send()


def per_device(
    tokens,
    old_state,
    w_query,
    w_forget,
    w_value,
    w_gate,
    lower_bound,
    head_gain,
    w_out,
    mix_gain,
    expert_gate,
    expert_up,
    expert_down,
    expert_ids,
    route_weight,
    moe_gain,
):
    n_ep = lax.axis_size("ep")
    rows, width = tokens.shape
    heads = old_state.shape[1]
    cols = w_query.shape[1]
    units = expert_gate.shape[2]
    half = width // 2
    blocks = half // 128
    n_slots = 2 * n_ep
    tall = rows * heads
    anywhere = pl.BlockSpec(memory_space=pl.ANY)
    vmem = pl.BlockSpec(memory_space=pltpu.VMEM)
    message = pltpu.VMEM((blocks, n_ep, 2, 128), BF)
    down = pltpu.VMEM((n_slots, half), BF)
    by_head = pltpu.VMEM((tall, 128), F32)
    row = pltpu.VMEM((rows, width), BF)
    return pl.pallas_call(
        kernel,
        out_shape=(
            pltpu.VMEM((rows, half), BF),
            pltpu.VMEM(old_state.shape, F32),
        ),
        in_specs=[anywhere] * 16,
        out_specs=(vmem, vmem),
        scratch_shapes=[
            row,
            *[pltpu.VMEM((width, cols), BF)] * 4,
            pltpu.VMEM((cols, width), BF),
            pltpu.VMEM((width, units), BF),
            pltpu.VMEM((width, units), BF),
            pltpu.VMEM((units, width), BF),
            pltpu.VMEM((1, cols), F32),
            pltpu.VMEM((1, head_gain.shape[0]), F32),
            pltpu.VMEM((1, width), F32),
            pltpu.VMEM((2, rows), jnp.int32),
            pltpu.VMEM((2, rows), F32),
            pltpu.VMEM((1, width), F32),
            by_head,
            by_head,
            by_head,
            by_head,
            pltpu.VMEM((2 * tall, 256), BF),
            pltpu.VMEM((rows, cols), BF),
            row,
            row,
            row,
            message,
            message,
            message,
            down,
            down,
            down,
            message,
            message,
            pltpu.VMEM((rows, 128), F32),
            pltpu.VMEM((rows, 128), F32),
            pltpu.VMEM((8, 128), F32),
            pltpu.SemaphoreType.DMA((19,)),
            pltpu.SemaphoreType.DMA((10,)),
            pltpu.SemaphoreType.DMA((10,)),
            pltpu.SemaphoreType.DMA((2,)),
            pltpu.SemaphoreType.DMA((8,)),
        ],
        compiler_params=pltpu.CompilerParams(
            collective_id=0, has_side_effects=True, vmem_limit_bytes=56 * 1024 * 1024
        ),
    )(
        tokens,
        old_state,
        w_query,
        w_forget,
        w_value,
        w_gate,
        lower_bound.reshape(1, cols),
        head_gain.reshape(1, -1),
        w_out,
        mix_gain.reshape(1, width),
        expert_gate,
        expert_up,
        expert_down,
        expert_ids.T,
        route_weight.T,
        moe_gain.reshape(1, width),
    )


def solution(mesh):
    in_specs = (
        P("ep", None),
        P("ep", "tp", None),
        P(None, "tp"),
        P(None, "tp"),
        P(None, "tp"),
        P(None, "tp"),
        P("tp"),
        P(),
        P("tp", None),
        P(),
        P("ep", None, "tp"),
        P("ep", None, "tp"),
        P("ep", "tp", None),
        P("ep", None),
        P("ep", None),
        P(),
    )
    out_specs = (P("ep", "tp"), P("ep", "tp", None))
    return jax.shard_map(
        per_device, mesh=mesh, in_specs=in_specs, out_specs=out_specs, check_vma=False
    )
```

```python
import jax
import jax.numpy as jnp
from jax import lax
from jax.experimental import pallas as pl
from jax.experimental.pallas import tpu as pltpu
from jax.sharding import PartitionSpec as P

MESH = pl.DeviceIdType.MESH
BF = jnp.bfloat16
F32 = jnp.float32


def dot(a, b):
    return jnp.dot(a, b, preferred_element_type=F32)


def silu(v):
    return v / (1.0 + jnp.exp(-v))


AXES = (8, 4, 4)
CHIPS = AXES[1] * AXES[2]
PLANE = CHIPS // 2
Z_ORDER = (3, 5, 2, 6, 4, 1, 7, 0)
GROUPS = ((0, 2), (2, 4), (4, 5), (5, 8))
HOME = Z_ORDER.index(0)
SELF = HOME * PLANE


def kernel(
    tokens,
    old,
    w_query,
    w_forget,
    w_value,
    w_gate,
    bound_in,
    head_gain_in,
    w_out,
    mix_gain_in,
    e_gate,
    e_up,
    e_down,
    ids_in,
    weight_in,
    moe_gain_in,
    next_out,
    st,
    tok,
    wq,
    wf,
    wv,
    wg,
    wo,
    eg,
    eu,
    ed,
    eg_far,
    eu_far,
    ed_far,
    bound,
    head_gain,
    mix_gain,
    ids,
    weight,
    moe_gain,
    f_s,
    q_s,
    v_s,
    r_s,
    gates,
    mix,
    own_part,
    other_part,
    after,
    send,
    recv,
    ret_send,
    ret_recv,
    own_moe,
    other_moe,
    small,
    in_sem,
    tp_send,
    tp_recv,
    ep_send,
    ep_recv,
):
    me = lax.axis_index("ep")
    core = lax.axis_index("tp")
    rows, width = tok.shape
    heads = st.shape[1]
    half = width // 2
    blocks = width // 128
    own_cols = pl.multiple_of(core * half, 128)
    slots = AXES[0] * PLANE
    n_keys = st.shape[2]
    my_z = lax.div(me, CHIPS)
    my_y = lax.rem(lax.div(me, AXES[2]), AXES[1])
    my_x = lax.rem(me, AXES[2])
    z_at = [lax.rem(my_z + dz, AXES[0]) * CHIPS for dz in range(AXES[0])]
    x_at = {
        (sign, q): lax.rem(my_x + AXES[2] + sign * (2 * q + core), AXES[2])
        for sign in (1, -1)
        for q in (0, 1)
    }

    def each_of_plane(pos, sign, visit):
        dz = Z_ORDER[pos]
        base = z_at[(sign * dz) % AXES[0]]

        def one(dy, q):
            y = my_y + dy if sign > 0 else my_y + AXES[1] - dy
            y = jnp.where(y >= AXES[1], y - AXES[1], y) * AXES[2]
            visit(pos * PLANE + dy * 2 + q, base + y + x_at[sign, q])

        def body(dy, carry):
            one(dy, 0)
            one(dy, 1)
            return carry

        if dz == 0:

            @pl.when(core == 1)
            def _():
                one(0, 0)

            one(0, 1)
        lax.fori_loop(1 if dz == 0 else 0, AXES[1], body, 0)

    part = n_keys // 4
    pieces = [
        (tokens, tok),
        (bound_in, bound),
        (w_forget, wf),
        (w_query, wq),
        (w_value, wv),
        *((old.at[:, :, pl.ds(i * part, part)], st.at[:, :, pl.ds(i * part, part)]) for i in range(4)),
        (w_gate, wg),
        (head_gain_in, head_gain),
        (w_out, wo),
        (mix_gain_in, mix_gain),
        (ids_in, ids),
        (weight_in, weight),
        (e_gate.at[0], eg),
        (e_up.at[0], eu),
        (e_down.at[0], ed),
        (moe_gain_in, moe_gain),
    ]
    loads = [pltpu.make_async_copy(src, dst, in_sem.at[i]) for i, (src, dst) in enumerate(pieces)]
    for load in loads:
        load.start()
    l_tok, l_bound, l_wf, l_wq, l_wv = loads[:5]
    l_state = loads[5:9]
    l_wg, l_hg, l_wo, l_mg, l_ids, l_weight, l_eg, l_eu, l_ed, l_og = loads[9:]

    barrier = pltpu.get_barrier_semaphore()
    pl.semaphore_signal(barrier, inc=1, device_id=(me, 1 - core), device_id_type=MESH)

    def greet(slot, peer):
        pl.semaphore_signal(barrier, inc=1, device_id=(peer, core), device_id_type=MESH)

    for dz in (4, 3, 5, 2, 6, 1, 7, 0):
        each_of_plane(Z_ORDER.index(dz), 1, greet)

    pairs = heads // 2
    tall = rows * heads

    def by_head(ref, values, p):
        ref[pl.ds(2 * p, rows, heads), :] = values
        ref[pl.ds(2 * p + 1, rows, heads), :] = values

    lane = lax.broadcasted_iota(jnp.int32, (tall, 128), 1)
    head = lax.broadcasted_iota(jnp.int32, (tall, 128), 0)
    mine = lax.shift_right_logical(lane, 6) == lax.bitwise_and(head, 1)

    def split(ref, first):
        values = jnp.where(mine, ref[...], 0.0)
        high = values.astype(BF)
        gates[first : first + tall, 0:128] = high
        gates[first : first + tall, 128:256] = (values - high.astype(F32)).astype(BF)

    l_tok.wait()
    x = tok[...]
    l_bound.wait()
    l_wf.wait()
    f_lin = dot(x, wf[...])
    for p in range(pairs):
        cols = slice(p * 128, (p + 1) * 128)
        low = bound[:, cols]
        by_head(f_s, low + (1.0 - low) / (1.0 + jnp.exp(-f_lin[:, cols])), p)
    split(f_s, 0)
    l_wq.wait()
    q_lin = dot(x, wq[...])
    for p in range(pairs):
        by_head(q_s, silu(q_lin[:, p * 128 : (p + 1) * 128]), p)
    split(q_s, tall)
    l_wv.wait()
    v_lin = dot(x, wv[...])
    for p in range(pairs):
        by_head(v_s, v_lin[:, p * 128 : (p + 1) * 128], p)
    v_pair = v_s[...]
    v_s[...] = jnp.where(mine, v_pair, pltpu.roll(v_pair, 64, 1))
    r_s[...] = jnp.zeros_like(r_s)

    tile = 256
    key_gap = (
        lax.bitwise_and(lax.broadcasted_iota(jnp.int32, (tile, tile), 0), 63)
        - lax.shift_right_logical(lax.broadcasted_iota(jnp.int32, (tile, tile), 1), 6)
    ).astype(F32)

    def one_tile(n):
        spread = jnp.where(key_gap == 4.0 * n, 1.0, 0.0).astype(BF)
        both = dot(gates[...], spread)
        cols = slice(n * tile, (n + 1) * tile)
        previous = st[:, :, cols].reshape(tall, tile)
        value = jnp.concatenate([v_s[...], v_s[...]], axis=1)
        new = value + both[:tall] * (previous - value)
        st[:, :, cols] = new.reshape(rows, heads, tile)
        read = both[tall:] * new
        return read[:, :128] + read[:, 128:]

    per_part = part // tile
    for i in range(4):
        l_state[i].wait()
        for n in range(i * per_part, (i + 1) * per_part):
            r_s[...] += one_tile(n)
    r_s[...] += pltpu.roll(r_s[...], 64, 1)

    l_wg.wait()
    l_hg.wait()
    g_lin = dot(x, wg[...])
    first_head = lax.broadcasted_iota(jnp.int32, (rows, 128), 1) < 64
    gain2 = jnp.concatenate([head_gain[...], head_gain[...]], axis=1)
    for p in range(pairs):
        cols = slice(p * 128, (p + 1) * 128)
        even_head = r_s[pl.ds(2 * p, rows, heads), :]
        odd_head = r_s[pl.ds(2 * p + 1, rows, heads), :]
        even_head = even_head * lax.rsqrt(
            jnp.sum(even_head * even_head, -1, keepdims=True) / 128.0 + 1e-6
        )
        odd_head = odd_head * lax.rsqrt(
            jnp.sum(odd_head * odd_head, -1, keepdims=True) / 128.0 + 1e-6
        )
        normed = jnp.where(first_head, even_head, odd_head) * gain2
        mix[:, cols] = (normed * silu(g_lin[:, cols])).astype(BF)
    l_wo.wait()
    own_part[...] = dot(mix[...], wo[...]).astype(BF)

    pl.semaphore_wait(barrier, slots + core)

    def to_partner(src, dst, i):
        return pltpu.make_async_remote_copy(
            src_ref=src,
            dst_ref=dst,
            send_sem=tp_send.at[i],
            recv_sem=tp_recv.at[i],
            device_id=(me, 1 - core),
            device_id_type=MESH,
        )

    swap = to_partner(own_part, other_part, 0)
    swap.start()

    for load in (l_eg, l_eu, l_ed):
        load.wait()
    halves = [to_partner(eg, eg_far, 1), to_partner(eu, eu_far, 2), to_partner(ed, ed_far, 3)]
    for push in halves:
        push.start()

    for load in (l_ids, l_weight, l_mg):
        load.wait()
    small[...] = jnp.zeros_like(small)
    small[0:2, 0:rows] = ids[...].astype(F32)
    small[2:4, 0:rows] = weight[...]
    turned = small[...].T[0:rows]
    id0 = turned[:, 0:1].astype(jnp.int32)
    id1 = turned[:, 1:2].astype(jnp.int32)
    slot_iota = lax.broadcasted_iota(jnp.int32, (rows, 2 * slots), 1)
    slot_pos = lax.shift_right_logical(slot_iota, 4)
    dz = jnp.zeros_like(slot_pos)
    for pos, offset in enumerate(Z_ORDER):
        dz = jnp.where(slot_pos == pos, offset, dz)
    dy = lax.bitwise_and(lax.shift_right_logical(slot_iota, 2), 3)
    dx = lax.bitwise_and(slot_iota, 2) + core
    expert = (
        lax.bitwise_and(my_z + dz, 7) * CHIPS
        + lax.bitwise_and(my_y + dy, 3) * AXES[2]
        + lax.bitwise_and(my_x + dx, 3)
    )
    names0 = expert == id0
    names1 = expert == id1
    named = jnp.where(names0 | names1, 1.0, 0.0)
    r_iota = lax.broadcasted_iota(jnp.int32, (rows, rows), 0)
    c_iota = lax.broadcasted_iota(jnp.int32, (rows, rows), 1)
    earlier = jnp.where(c_iota < r_iota, 1.0, 0.0)
    rank = dot(earlier.astype(BF), named.astype(BF))
    slot_of = lax.bitwise_and(slot_iota, 1).astype(F32)
    takes = jnp.where(rank == slot_of, named, 0.0)
    route = jnp.where(names0, turned[:, 2:3], 0.0) + jnp.where(names1, turned[:, 3:4], 0.0)
    route = jnp.where(rank == slot_of, route, 0.0)
    route_high = route.astype(BF)
    route_low = (route - route_high.astype(F32)).astype(BF)
    route_both = jnp.concatenate([route_high.astype(F32), route_low.astype(F32)], axis=0).astype(BF)
    choose = takes.T.astype(BF)
    swap.wait()
    mixed = own_part[...].astype(F32) + other_part[...].astype(F32)
    full = x.astype(F32) + mixed
    centered = full - jnp.mean(full, -1, keepdims=True)
    variance = jnp.mean(centered * centered, -1, keepdims=True)
    after[...] = (centered * lax.rsqrt(variance + 1e-5) * mix_gain[...]).astype(BF)

    def exchange(src, dst, send_sem, recv_sem, group, sign):
        def give(slot, peer):
            pltpu.make_async_remote_copy(
                src_ref=src.at[:, slot],
                dst_ref=dst.at[:, slot],
                send_sem=send_sem,
                recv_sem=recv_sem,
                device_id=(peer, core),
                device_id_type=MESH,
            ).start()

        for pos in range(*group):
            each_of_plane(pos, sign, give)
        if group[0] <= HOME < group[1]:

            @pl.when(core == 0)
            def _():
                dst[:, SELF : SELF + 1] = src[:, SELF : SELF + 1]

    def bytes_of(src, dst, send_sem, recv_sem, first, count):
        return pltpu.make_async_remote_copy(
            src_ref=src.at[:, pl.ds(first, count)],
            dst_ref=dst.at[:, pl.ds(first, count)],
            send_sem=send_sem,
            recv_sem=recv_sem,
            device_id=(me, 1 - core),
            device_id_type=MESH,
        )

    def span(group):
        return group[0] * PLANE, group[1] * PLANE

    def arrived(src, dst, send_sem, recv_sem, group):
        first, last = span(group)
        if group[0] <= HOME < group[1]:

            @pl.when(core == 0)
            def _():
                bytes_of(src, dst, send_sem, recv_sem, first, last - first - 1).wait_recv()

            @pl.when(core == 1)
            def _():
                bytes_of(src, dst, send_sem, recv_sem, first, last - first).wait_recv()

        else:
            bytes_of(src, dst, send_sem, recv_sem, first, last - first).wait_recv()

    def put_rows(buf, values, first, last):
        for j in range(blocks):
            buf[j, first:last] = values[:, j * 128 : (j + 1) * 128].reshape(last - first, 2, 128)

    def rows_of(buf, first, last):
        return jnp.concatenate(
            [buf[j, first:last].reshape(2 * (last - first), 128) for j in range(blocks)], axis=1
        )

    for g, group in enumerate(GROUPS):
        first, last = span(group)
        put_rows(send, dot(choose[2 * first : 2 * last], after[...]).astype(BF), first, last)
        exchange(send, recv, ep_send.at[0], ep_recv.at[g], group, 1)

    l_og.wait()
    for push in halves:
        push.wait_recv()

    for g, group in enumerate(GROUPS):
        first, last = span(group)
        arrived(send, recv, ep_send.at[0], ep_recv.at[g], group)
        inputs = rows_of(recv, first, last)
        hidden = (silu(dot(inputs, eg[...])) * dot(inputs, eu[...])).astype(BF)
        hidden_far = (silu(dot(inputs, eg_far[...])) * dot(inputs, eu_far[...])).astype(BF)
        result = dot(hidden, ed[...]).astype(BF).astype(F32)
        result_far = dot(hidden_far, ed_far[...]).astype(BF).astype(F32)
        put_rows(ret_send, (result + result_far).astype(BF), first, last)
        exchange(ret_send, ret_recv, ep_send.at[1], ep_recv.at[len(GROUPS) + g], group, -1)

    moe_sum = None
    for g, group in enumerate(GROUPS):
        first, last = span(group)
        arrived(ret_send, ret_recv, ep_send.at[1], ep_recv.at[len(GROUPS) + g], group)
        both = dot(route_both[:, 2 * first : 2 * last], rows_of(ret_recv, first, last))
        both = both[:rows] + both[rows:]
        moe_sum = both if moe_sum is None else moe_sum + both
    own_moe[...] = moe_sum
    last_swap = to_partner(own_moe, other_moe, 4)
    last_swap.start()
    last_swap.wait_recv()
    final = after[...].astype(F32) + (own_moe[...] + other_moe[...])
    centered = final - jnp.mean(final, -1, keepdims=True)
    scale = lax.rsqrt(jnp.mean(centered * centered, -1, keepdims=True) + 1e-5)
    other_moe[...] = centered * scale * moe_gain[...]
    next_out[...] = other_moe[:, pl.ds(own_cols, half)].astype(BF)

    @pl.when(core == 0)
    def _():
        bytes_of(send, recv, ep_send.at[0], ep_recv.at[0], 0, slots - 1).wait_send()
        bytes_of(ret_send, ret_recv, ep_send.at[1], ep_recv.at[0], 0, slots - 1).wait_send()

    @pl.when(core == 1)
    def _():
        bytes_of(send, recv, ep_send.at[0], ep_recv.at[0], 0, slots).wait_send()
        bytes_of(ret_send, ret_recv, ep_send.at[1], ep_recv.at[0], 0, slots).wait_send()

    for remote in (*halves, last_swap):
        remote.wait_send()


def per_device(
    tokens,
    old_state,
    w_query,
    w_forget,
    w_value,
    w_gate,
    lower_bound,
    head_gain,
    w_out,
    mix_gain,
    expert_gate,
    expert_up,
    expert_down,
    expert_ids,
    route_weight,
    moe_gain,
):
    n_ep = lax.axis_size("ep")
    rows, width = tokens.shape
    heads = old_state.shape[1]
    cols = w_query.shape[1]
    units = expert_gate.shape[2]
    half = width // 2
    tall = rows * heads
    anywhere = pl.BlockSpec(memory_space=pl.ANY)
    vmem = pl.BlockSpec(memory_space=pltpu.VMEM)
    message = pltpu.VMEM((width // 128, n_ep // 2, 2, 128), BF)
    by_head = pltpu.VMEM((tall, 128), F32)
    row = pltpu.VMEM((rows, width), BF)
    return pl.pallas_call(
        kernel,
        out_shape=(
            pltpu.VMEM((rows, half), BF),
            pltpu.VMEM(old_state.shape, F32),
        ),
        in_specs=[anywhere] * 16,
        out_specs=(vmem, vmem),
        scratch_shapes=[
            row,
            *[pltpu.VMEM((width, cols), BF)] * 4,
            pltpu.VMEM((cols, width), BF),
            *[pltpu.VMEM((width, units), BF), pltpu.VMEM((width, units), BF), pltpu.VMEM((units, width), BF)] * 2,
            pltpu.VMEM((1, cols), F32),
            pltpu.VMEM((1, head_gain.shape[0]), F32),
            pltpu.VMEM((1, width), F32),
            pltpu.VMEM((2, rows), jnp.int32),
            pltpu.VMEM((2, rows), F32),
            pltpu.VMEM((1, width), F32),
            by_head,
            by_head,
            by_head,
            by_head,
            pltpu.VMEM((2 * tall, 256), BF),
            pltpu.VMEM((rows, cols), BF),
            row,
            row,
            row,
            message,
            message,
            message,
            message,
            pltpu.VMEM((rows, width), F32),
            pltpu.VMEM((rows, width), F32),
            pltpu.VMEM((8, 128), F32),
            pltpu.SemaphoreType.DMA((19,)),
            pltpu.SemaphoreType.DMA((5,)),
            pltpu.SemaphoreType.DMA((5,)),
            pltpu.SemaphoreType.DMA((2,)),
            pltpu.SemaphoreType.DMA((2 * len(GROUPS),)),
        ],
        compiler_params=pltpu.CompilerParams(
            collective_id=0, has_side_effects=True, vmem_limit_bytes=56 * 1024 * 1024
        ),
    )(
        tokens,
        old_state,
        w_query,
        w_forget,
        w_value,
        w_gate,
        lower_bound.reshape(1, cols),
        head_gain.reshape(1, -1),
        w_out,
        mix_gain.reshape(1, width),
        expert_gate,
        expert_up,
        expert_down,
        expert_ids.T,
        route_weight.T,
        moe_gain.reshape(1, width),
    )


def solution(mesh):
    in_specs = (
        P("ep", None),
        P("ep", "tp", None),
        P(None, "tp"),
        P(None, "tp"),
        P(None, "tp"),
        P(None, "tp"),
        P("tp"),
        P(),
        P("tp", None),
        P(),
        P("ep", None, "tp"),
        P("ep", None, "tp"),
        P("ep", "tp", None),
        P("ep", None),
        P("ep", None),
        P(),
    )
    out_specs = (P("ep", "tp"), P("ep", "tp", None))
    return jax.shard_map(
        per_device, mesh=mesh, in_specs=in_specs, out_specs=out_specs, check_vma=False
    )
```

```python
import jax
import jax.numpy as jnp
from jax import lax
from jax.experimental import pallas as pl
from jax.experimental.pallas import tpu as pltpu
from jax.sharding import PartitionSpec as P

MESH = pl.DeviceIdType.MESH
BF = jnp.bfloat16
F32 = jnp.float32


def dot(a, b):
    return jnp.dot(a, b, preferred_element_type=F32)


def silu(v):
    return v / (1.0 + jnp.exp(-v))


AXES = (8, 4, 4)
CHIPS = AXES[1] * AXES[2]
PLANE = CHIPS // 2
FAR = ((4,),)
Z_ORDER = (3, 5, 2, 6, 1, 7, 0)
GROUPS = ((0, 2), (2, 4), (4, 7))
HOME = Z_ORDER.index(0)
SELF = HOME * PLANE
RING = AXES[2]
WIDE = 4


def kernel(
    tokens,
    old,
    w_query,
    w_forget,
    w_value,
    w_gate,
    bound_in,
    head_gain_in,
    w_out,
    mix_gain_in,
    e_gate,
    e_up,
    e_down,
    ids_in,
    weight_in,
    total_out,
    st,
    tok,
    wq,
    wf,
    wv,
    wg,
    wo,
    eg,
    eu,
    ed,
    eg_far,
    eu_far,
    ed_far,
    bound,
    head_gain,
    mix_gain,
    ids,
    weight,
    f_s,
    q_s,
    v_s,
    r_s,
    gates,
    mix,
    own_part,
    other_part,
    after,
    send,
    recv,
    ret_send,
    ret_recv,
    far_refs,
    own_moe,
    other_moe,
    small,
    in_sem,
    tp_send,
    tp_recv,
    ep_send,
    ep_recv,
    far_send_sem,
    far_recv_sem,
):
    me = lax.axis_index("ep")
    core = lax.axis_index("tp")
    rows, width = tok.shape
    heads = st.shape[1]
    blocks = width // 128
    slots = len(Z_ORDER) * PLANE
    n_keys = st.shape[2]
    my_z = lax.div(me, CHIPS)
    my_y = lax.rem(lax.div(me, AXES[2]), AXES[1])
    my_x = lax.rem(me, AXES[2])
    z_at = [lax.rem(my_z + dz, AXES[0]) * CHIPS for dz in range(AXES[0])]
    x_at = {
        (sign, q): lax.rem(my_x + AXES[2] + sign * (2 * q + core), AXES[2])
        for sign in (1, -1)
        for q in (0, 1)
    }

    def far_peers(g, sign):
        for i, dz in enumerate(FAR[g]):
            for h in range(2):
                y = lax.rem(my_y + AXES[1] + sign * (2 * h + core), AXES[1])
                yield 2 * i + h, z_at[(sign * dz) % AXES[0]] + y * AXES[2] + my_x

    def ring_peer(dx):
        return me - my_x + lax.rem(my_x + AXES[2] + dx, AXES[2])

    def each_of_plane(pos, sign, visit):
        dz = Z_ORDER[pos]
        base = z_at[(sign * dz) % AXES[0]]

        def one(dy, q):
            y = my_y + dy if sign > 0 else my_y + AXES[1] - dy
            y = jnp.where(y >= AXES[1], y - AXES[1], y) * AXES[2]
            visit(pos * PLANE + dy * 2 + q, base + y + x_at[sign, q])

        def body(dy, carry):
            one(dy, 0)
            one(dy, 1)
            return carry

        if dz == 0:

            @pl.when(core == 1)
            def _():
                one(0, 0)

            one(0, 1)
        lax.fori_loop(1 if dz == 0 else 0, AXES[1], body, 0)

    part = n_keys // 4
    pieces = [
        (tokens, tok),
        (bound_in, bound),
        (w_forget, wf),
        (w_query, wq),
        (w_value, wv),
        *((old.at[:, :, pl.ds(i * part, part)], st.at[:, :, pl.ds(i * part, part)]) for i in range(4)),
        (w_gate, wg),
        (head_gain_in, head_gain),
        (w_out, wo),
        (mix_gain_in, mix_gain),
        (ids_in, ids),
        (weight_in, weight),
        (e_gate.at[0], eg),
        (e_up.at[0], eu),
        (e_down.at[0], ed),
    ]
    loads = [pltpu.make_async_copy(src, dst, in_sem.at[i]) for i, (src, dst) in enumerate(pieces)]
    for load in loads:
        load.start()
    l_tok, l_bound, l_wf, l_wq, l_wv = loads[:5]
    l_state = loads[5:9]
    l_wg, l_hg, l_wo, l_mg, l_ids, l_weight, l_eg, l_eu, l_ed = loads[9:]

    barrier = pltpu.get_barrier_semaphore()
    pl.semaphore_signal(barrier, inc=1, device_id=(me, 1 - core), device_id_type=MESH)

    def greet(slot, peer):
        pl.semaphore_signal(barrier, inc=1, device_id=(peer, core), device_id_type=MESH)

    for g in range(len(FAR)):
        for slot, peer in far_peers(g, 1):
            greet(slot, peer)
    for pos in range(len(Z_ORDER)):
        each_of_plane(pos, 1, greet)
    for dx in range(1, RING):
        greet(dx, ring_peer(dx))

    pairs = heads // 2
    tall = rows * heads

    def by_head(ref, values, p):
        ref[pl.ds(2 * p, rows, heads), :] = values
        ref[pl.ds(2 * p + 1, rows, heads), :] = values

    lane = lax.broadcasted_iota(jnp.int32, (tall, 128), 1)
    head = lax.broadcasted_iota(jnp.int32, (tall, 128), 0)
    mine = lax.shift_right_logical(lane, 6) == lax.bitwise_and(head, 1)

    def split(ref, first):
        values = jnp.where(mine, ref[...], 0.0)
        high = values.astype(BF)
        gates[first : first + tall, 0:128] = high
        gates[first : first + tall, 128:256] = (values - high.astype(F32)).astype(BF)

    l_tok.wait()
    x = tok[...]
    l_bound.wait()
    l_wf.wait()
    f_lin = dot(x, wf[...])
    for p in range(pairs):
        cols = slice(p * 128, (p + 1) * 128)
        low = bound[:, cols]
        by_head(f_s, low + (1.0 - low) / (1.0 + jnp.exp(-f_lin[:, cols])), p)
    split(f_s, 0)
    l_wq.wait()
    q_lin = dot(x, wq[...])
    for p in range(pairs):
        by_head(q_s, silu(q_lin[:, p * 128 : (p + 1) * 128]), p)
    split(q_s, tall)
    l_wv.wait()
    v_lin = dot(x, wv[...])
    for p in range(pairs):
        by_head(v_s, v_lin[:, p * 128 : (p + 1) * 128], p)
    v_pair = v_s[...]
    v_s[...] = jnp.where(mine, v_pair, pltpu.roll(v_pair, 64, 1))
    r_s[...] = jnp.zeros_like(r_s)

    tile = 256
    key_gap = (
        lax.bitwise_and(lax.broadcasted_iota(jnp.int32, (tile, tile), 0), 63)
        - lax.shift_right_logical(lax.broadcasted_iota(jnp.int32, (tile, tile), 1), 6)
    ).astype(F32)

    def one_tile(n):
        spread = jnp.where(key_gap == 4.0 * n, 1.0, 0.0).astype(BF)
        both = dot(gates[...], spread)
        cols = slice(n * tile, (n + 1) * tile)
        previous = st[:, :, cols].reshape(tall, tile)
        value = jnp.concatenate([v_s[...], v_s[...]], axis=1)
        new = value + both[:tall] * (previous - value)
        st[:, :, cols] = new.reshape(rows, heads, tile)
        read = both[tall:] * new
        return read[:, :128] + read[:, 128:]

    per_part = part // tile
    for i in range(4):
        l_state[i].wait()
        for n in range(i * per_part, (i + 1) * per_part):
            r_s[...] += one_tile(n)
    r_s[...] += pltpu.roll(r_s[...], 64, 1)

    l_wg.wait()
    l_hg.wait()
    g_lin = dot(x, wg[...])
    first_head = lax.broadcasted_iota(jnp.int32, (rows, 128), 1) < 64
    gain2 = jnp.concatenate([head_gain[...], head_gain[...]], axis=1)
    for p in range(pairs):
        cols = slice(p * 128, (p + 1) * 128)
        even_head = r_s[pl.ds(2 * p, rows, heads), :]
        odd_head = r_s[pl.ds(2 * p + 1, rows, heads), :]
        even_head = even_head * lax.rsqrt(
            jnp.sum(even_head * even_head, -1, keepdims=True) / 128.0 + 1e-6
        )
        odd_head = odd_head * lax.rsqrt(
            jnp.sum(odd_head * odd_head, -1, keepdims=True) / 128.0 + 1e-6
        )
        normed = jnp.where(first_head, even_head, odd_head) * gain2
        mix[:, cols] = (normed * silu(g_lin[:, cols])).astype(BF)
    l_wo.wait()
    own_part[...] = dot(mix[...], wo[...]).astype(BF)

    n_far = sum(2 * len(group) for group in FAR)
    pl.semaphore_wait(barrier, slots + core + n_far + RING - 1)

    def to_partner(src, dst, i):
        return pltpu.make_async_remote_copy(
            src_ref=src,
            dst_ref=dst,
            send_sem=tp_send.at[i],
            recv_sem=tp_recv.at[i],
            device_id=(me, 1 - core),
            device_id_type=MESH,
        )

    swap = to_partner(own_part, other_part, 0)
    swap.start()

    for load in (l_eg, l_eu, l_ed):
        load.wait()
    halves = [to_partner(eg, eg_far, 1), to_partner(eu, eu_far, 2), to_partner(ed, ed_far, 3)]
    for push in halves:
        push.start()

    for load in (l_ids, l_weight, l_mg):
        load.wait()
    small[...] = jnp.zeros_like(small)
    small[0:2, 0:rows] = ids[...].astype(F32)
    small[2:4, 0:rows] = weight[...]
    turned = small[...].T[0:rows]
    id0 = turned[:, 0:1].astype(jnp.int32)
    id1 = turned[:, 1:2].astype(jnp.int32)
    slot_iota = lax.broadcasted_iota(jnp.int32, (rows, 128), 1)
    slot_pos = lax.shift_right_logical(slot_iota, 4)
    dz = jnp.zeros_like(slot_pos)
    for pos, offset in enumerate(Z_ORDER):
        dz = jnp.where(slot_pos == pos, offset, dz)
    dy = lax.bitwise_and(lax.shift_right_logical(slot_iota, 2), 3)
    dx = lax.bitwise_and(slot_iota, 2) + core
    expert = (
        lax.bitwise_and(my_z + dz, 7) * CHIPS
        + lax.bitwise_and(my_y + dy, 3) * AXES[2]
        + lax.bitwise_and(my_x + dx, 3)
    )
    names0 = expert == id0
    names1 = expert == id1
    named = jnp.where(names0 | names1, 1.0, 0.0)
    r_iota = lax.broadcasted_iota(jnp.int32, (rows, rows), 0)
    c_iota = lax.broadcasted_iota(jnp.int32, (rows, rows), 1)
    earlier = jnp.where(c_iota < r_iota, 1.0, 0.0)
    rank = dot(earlier.astype(BF), named.astype(BF))
    slot_of = lax.bitwise_and(slot_iota, 1).astype(F32)
    takes = jnp.where(rank == slot_of, named, 0.0)
    route = jnp.where(names0, turned[:, 2:3], 0.0) + jnp.where(names1, turned[:, 3:4], 0.0)
    route = jnp.where(rank == slot_of, route, 0.0)
    route_high = route.astype(BF)
    route_low = (route - route_high.astype(F32)).astype(BF)
    route_both = jnp.concatenate([route_high.astype(F32), route_low.astype(F32)], axis=0).astype(BF)
    choose = takes.T.astype(BF)

    ring_of = lax.shift_right_logical(id0, 2)
    far_takes = []
    for group in FAR:
        far_pos = lax.shift_right_logical(slot_iota, 3)
        dz = jnp.zeros_like(far_pos)
        for i, offset in enumerate(group):
            dz = jnp.where(far_pos == i, offset, dz)
        dy = lax.bitwise_and(lax.shift_right_logical(slot_iota, 1), 2) + core
        ring = lax.bitwise_and(my_z + dz, 7) * AXES[1] + lax.bitwise_and(my_y + dy, 3)
        named = jnp.where(ring == ring_of, 1.0, 0.0)
        rank = dot(earlier.astype(BF), named.astype(BF))
        named = jnp.where(rank == lax.bitwise_and(slot_iota, 3).astype(F32), named, 0.0)
        far_takes.append(named)
    far_choose = [named.T.astype(BF) for named in far_takes]
    x_of = lax.bitwise_and(slot_iota, 3)
    ring_weight = jnp.where(x_of == lax.bitwise_and(id0, 3), turned[:, 2:3], 0.0) + jnp.where(
        x_of == lax.bitwise_and(id1, 3), turned[:, 3:4], 0.0
    )
    weight_high = ring_weight.astype(BF)
    weight_low = (ring_weight - weight_high.astype(F32)).astype(BF)
    weight_terms = jnp.where(
        slot_iota < 4, weight_high.astype(F32), jnp.where(slot_iota < 8, weight_low.astype(F32), 0.0)
    ).astype(BF)
    swap.wait()
    mixed = own_part[...].astype(F32) + other_part[...].astype(F32)
    full = x.astype(F32) + mixed
    centered = full - jnp.mean(full, -1, keepdims=True)
    variance = jnp.mean(centered * centered, -1, keepdims=True)
    after[...] = (centered * lax.rsqrt(variance + 1e-5) * mix_gain[...]).astype(BF)

    def exchange(src, dst, send_sem, recv_sem, group, sign):
        def give(slot, peer):
            pltpu.make_async_remote_copy(
                src_ref=src.at[:, slot],
                dst_ref=dst.at[:, slot],
                send_sem=send_sem,
                recv_sem=recv_sem,
                device_id=(peer, core),
                device_id_type=MESH,
            ).start()

        for pos in range(*group):
            each_of_plane(pos, sign, give)
        if group[0] <= HOME < group[1]:

            @pl.when(core == 0)
            def _():
                dst[:, SELF : SELF + 1] = src[:, SELF : SELF + 1]

    def bytes_of(src, dst, send_sem, recv_sem, first, count):
        return pltpu.make_async_remote_copy(
            src_ref=src.at[:, pl.ds(first, count)],
            dst_ref=dst.at[:, pl.ds(first, count)],
            send_sem=send_sem,
            recv_sem=recv_sem,
            device_id=(me, 1 - core),
            device_id_type=MESH,
        )

    def span(group):
        return group[0] * PLANE, group[1] * PLANE

    def arrived(src, dst, send_sem, recv_sem, group):
        first, last = span(group)
        if group[0] <= HOME < group[1]:

            @pl.when(core == 0)
            def _():
                bytes_of(src, dst, send_sem, recv_sem, first, last - first - 1).wait_recv()

            @pl.when(core == 1)
            def _():
                bytes_of(src, dst, send_sem, recv_sem, first, last - first).wait_recv()

        else:
            bytes_of(src, dst, send_sem, recv_sem, first, last - first).wait_recv()

    def put_rows(buf, values, first, last):
        for j in range(blocks):
            buf[j, first:last] = values[:, j * 128 : (j + 1) * 128].reshape(last - first, 2, 128)

    def rows_of(buf, first, last):
        return jnp.concatenate(
            [buf[j, first:last].reshape(2 * (last - first), 128) for j in range(blocks)], axis=1
        )

    def expert(inputs):
        hidden = (silu(dot(inputs, eg[...])) * dot(inputs, eu[...])).astype(BF)
        hidden_far = (silu(dot(inputs, eg_far[...])) * dot(inputs, eu_far[...])).astype(BF)
        result = dot(hidden, ed[...]).astype(BF).astype(F32)
        result_far = dot(hidden_far, ed_far[...]).astype(BF).astype(F32)
        return (result + result_far).astype(BF)

    def far_copy(src, dst, kind, g, peer):
        at = kind * len(FAR) + g
        return pltpu.make_async_remote_copy(
            src_ref=src,
            dst_ref=dst,
            send_sem=far_send_sem.at[at],
            recv_sem=far_recv_sem.at[at],
            device_id=(peer, core),
            device_id_type=MESH,
        )

    def far_dispatch(g):
        out, arrive = far_refs[g][0:2]
        n = out.shape[1]
        picked = dot(far_choose[g][: WIDE * n], after[...]).astype(BF)
        for j in range(blocks):
            out[j] = picked[:, j * 128 : (j + 1) * 128].reshape(n, WIDE, 128)
        out[blocks] = dot(far_choose[g][: WIDE * n], weight_terms).astype(BF).reshape(n, WIDE, 128)
        for slot, peer in far_peers(g, 1):
            far_copy(out.at[:, slot], arrive.at[:, slot], 0, g, peer).start()

    def far_hand_round(g):
        out, arrive, ring_in = far_refs[g][0:3]
        far_copy(out, arrive, 0, g, ring_peer(1)).wait_recv()
        for dx in range(1, RING):
            far_copy(arrive, ring_in.at[:, dx], 1, g, ring_peer(dx)).start()
        ring_in[:, 0] = arrive[...]

    def far_expert(g):
        ring_in, back, back_in = far_refs[g][2:5]
        n = ring_in.shape[2]
        count = RING * n * WIDE
        rest = pl.ds(1, RING - 1)
        far_copy(ring_in.at[:, rest], ring_in.at[:, rest], 1, g, ring_peer(1)).wait_recv()
        inputs = jnp.concatenate(
            [ring_in[j].reshape(count, 128) for j in range(blocks)], axis=1
        )
        terms = ring_in[blocks].reshape(count, 128).astype(F32)
        at = lax.broadcasted_iota(jnp.int32, (count, 128), 1)
        mine = lax.bitwise_and(at, 3) == my_x
        scale = jnp.sum(jnp.where(mine, terms, 0.0), -1, keepdims=True)
        given = (expert(inputs).astype(F32) * scale).astype(BF)
        for j in range(blocks):
            back[j] = given[:, j * 128 : (j + 1) * 128].reshape(RING, n, WIDE, 128)
        for dx in range(1, RING):
            far_copy(back.at[:, dx], back_in.at[:, dx], 2, g, ring_peer(-dx)).start()
        back_in[:, 0] = back[:, 0]

    def far_sum(g):
        back_in, out, home = far_refs[g][4:7]
        n = out.shape[1]
        rest = pl.ds(1, RING - 1)
        far_copy(back_in.at[:, rest], back_in.at[:, rest], 2, g, ring_peer(1)).wait_recv()
        for j in range(blocks):
            parts = back_in[j].reshape(RING * n * WIDE, 128).astype(F32).reshape(RING, n * WIDE, 128)
            out[j] = jnp.sum(parts, axis=0).astype(BF).reshape(n, WIDE, 128)
        for slot, peer in far_peers(g, -1):
            far_copy(out.at[:, slot], home.at[:, slot], 3, g, peer).start()

    for g in range(len(FAR)):
        far_dispatch(g)
    for g, group in enumerate(GROUPS):
        first, last = span(group)
        put_rows(send, dot(choose[2 * first : 2 * last], after[...]).astype(BF), first, last)
        exchange(send, recv, ep_send.at[0], ep_recv.at[g], group, 1)

    def near_expert(g):
        group = GROUPS[g]
        first, last = span(group)
        arrived(send, recv, ep_send.at[0], ep_recv.at[g], group)
        put_rows(ret_send, expert(rows_of(recv, first, last)), first, last)
        exchange(ret_send, ret_recv, ep_send.at[1], ep_recv.at[len(GROUPS) + g], group, -1)

    far_hand_round(0)
    for push in halves:
        push.wait_recv()
    near_expert(0)
    far_expert(0)
    near_expert(1)
    far_sum(0)
    near_expert(2)

    moe_sum = None
    for g, group in enumerate(GROUPS):
        first, last = span(group)
        arrived(ret_send, ret_recv, ep_send.at[1], ep_recv.at[len(GROUPS) + g], group)
        both = dot(route_both[:, 2 * first : 2 * last], rows_of(ret_recv, first, last))
        both = both[:rows] + both[rows:]
        moe_sum = both if moe_sum is None else moe_sum + both
    for g in range(len(FAR)):
        out, home = far_refs[g][5:7]
        n = home.shape[1]
        far_copy(out, home, 3, g, ring_peer(1)).wait_recv()
        rows_back = jnp.concatenate(
            [home[j].reshape(n * WIDE, 128) for j in range(blocks)], axis=1
        )
        moe_sum = moe_sum + dot(far_takes[g][:, : n * WIDE].astype(BF), rows_back)
    own_moe[...] = moe_sum
    last_swap = to_partner(own_moe, other_moe, 4)
    last_swap.start()
    last_swap.wait_recv()
    total_out[...] = after[...].astype(F32) + (own_moe[...] + other_moe[...])

    @pl.when(core == 0)
    def _():
        bytes_of(send, recv, ep_send.at[0], ep_recv.at[0], 0, slots - 1).wait_send()
        bytes_of(ret_send, ret_recv, ep_send.at[1], ep_recv.at[0], 0, slots - 1).wait_send()

    @pl.when(core == 1)
    def _():
        bytes_of(send, recv, ep_send.at[0], ep_recv.at[0], 0, slots).wait_send()
        bytes_of(ret_send, ret_recv, ep_send.at[1], ep_recv.at[0], 0, slots).wait_send()

    for g in range(len(FAR)):
        out, arrive, ring_in, back, back_in, total, home = far_refs[g]
        rest = pl.ds(1, RING - 1)
        far_copy(out, arrive, 0, g, ring_peer(1)).wait_send()
        far_copy(ring_in.at[:, rest], ring_in.at[:, rest], 1, g, ring_peer(1)).wait_send()
        far_copy(back.at[:, rest], back_in.at[:, rest], 2, g, ring_peer(1)).wait_send()
        far_copy(total, home, 3, g, ring_peer(1)).wait_send()
    for remote in (*halves, last_swap):
        remote.wait_send()


def finish(total, state_in, moe_gain_in, next_out, state_out, moe_gain, normed, result, sem):
    core = lax.axis_index("tp")
    half = next_out.shape[1]
    parts = sem.shape[0] - 2
    rows = state_in.shape[0] // parts
    gain_load = pltpu.make_async_copy(moe_gain_in, moe_gain, sem.at[parts])
    gain_load.start()
    copies = [
        pltpu.make_async_copy(
            state_in.at[pl.ds(i * rows, rows)], state_out.at[pl.ds(i * rows, rows)], sem.at[i]
        )
        for i in range(parts)
    ]
    for copy in copies:
        copy.start()
    values = total[...]
    centered = values - jnp.mean(values, -1, keepdims=True)
    scale = lax.rsqrt(jnp.mean(centered * centered, -1, keepdims=True) + 1e-5)
    gain_load.wait()
    normed[...] = centered * scale * moe_gain[...]
    result[...] = normed[:, pl.ds(pl.multiple_of(core * half, 128), half)].astype(BF)
    copies.append(pltpu.make_async_copy(result, next_out, sem.at[parts + 1]))
    copies[-1].start()
    for copy in copies:
        copy.wait()


def per_device(
    tokens,
    old_state,
    w_query,
    w_forget,
    w_value,
    w_gate,
    lower_bound,
    head_gain,
    w_out,
    mix_gain,
    expert_gate,
    expert_up,
    expert_down,
    expert_ids,
    route_weight,
    moe_gain,
):
    rows, width = tokens.shape
    heads = old_state.shape[1]
    cols = w_query.shape[1]
    units = expert_gate.shape[2]
    half = width // 2
    tall = rows * heads
    anywhere = pl.BlockSpec(memory_space=pl.ANY)
    vmem = pl.BlockSpec(memory_space=pltpu.VMEM)
    blocks = width // 128
    message = pltpu.VMEM((blocks, len(Z_ORDER) * PLANE, 2, 128), BF)
    far = tuple(
        (
            pltpu.VMEM((blocks + 1, 2 * len(group), WIDE, 128), BF),
            pltpu.VMEM((blocks + 1, 2 * len(group), WIDE, 128), BF),
            pltpu.VMEM((blocks + 1, RING, 2 * len(group), WIDE, 128), BF),
            pltpu.VMEM((blocks, RING, 2 * len(group), WIDE, 128), BF),
            pltpu.VMEM((blocks, RING, 2 * len(group), WIDE, 128), BF),
            pltpu.VMEM((blocks, 2 * len(group), WIDE, 128), BF),
            pltpu.VMEM((blocks, 2 * len(group), WIDE, 128), BF),
        )
        for group in FAR
    )
    by_head = pltpu.VMEM((tall, 128), F32)
    row = pltpu.VMEM((rows, width), BF)
    total, new_state = pl.pallas_call(
        kernel,
        out_shape=(
            pltpu.VMEM((rows, width), F32),
            pltpu.VMEM(old_state.shape, F32),
        ),
        in_specs=[anywhere] * 15,
        out_specs=(vmem, vmem),
        scratch_shapes=[
            row,
            *[pltpu.VMEM((width, cols), BF)] * 4,
            pltpu.VMEM((cols, width), BF),
            *[pltpu.VMEM((width, units), BF), pltpu.VMEM((width, units), BF), pltpu.VMEM((units, width), BF)] * 2,
            pltpu.VMEM((1, cols), F32),
            pltpu.VMEM((1, head_gain.shape[0]), F32),
            pltpu.VMEM((1, width), F32),
            pltpu.VMEM((2, rows), jnp.int32),
            pltpu.VMEM((2, rows), F32),
            by_head,
            by_head,
            by_head,
            by_head,
            pltpu.VMEM((2 * tall, 256), BF),
            pltpu.VMEM((rows, cols), BF),
            row,
            row,
            row,
            message,
            message,
            message,
            message,
            far,
            pltpu.VMEM((rows, width), F32),
            pltpu.VMEM((rows, width), F32),
            pltpu.VMEM((8, 128), F32),
            pltpu.SemaphoreType.DMA((18,)),
            pltpu.SemaphoreType.DMA((5,)),
            pltpu.SemaphoreType.DMA((5,)),
            pltpu.SemaphoreType.DMA((2,)),
            pltpu.SemaphoreType.DMA((2 * len(GROUPS),)),
            pltpu.SemaphoreType.DMA((4 * len(FAR),)),
            pltpu.SemaphoreType.DMA((4 * len(FAR),)),
        ],
        compiler_params=pltpu.CompilerParams(
            collective_id=0, has_side_effects=True, vmem_limit_bytes=56 * 1024 * 1024
        ),
    )(
        tokens,
        old_state,
        w_query,
        w_forget,
        w_value,
        w_gate,
        lower_bound.reshape(1, cols),
        head_gain.reshape(1, -1),
        w_out,
        mix_gain.reshape(1, width),
        expert_gate,
        expert_up,
        expert_down,
        expert_ids.T,
        route_weight.T,
    )
    return pl.pallas_call(
        finish,
        out_shape=(
            jax.ShapeDtypeStruct((rows, half), BF),
            jax.ShapeDtypeStruct(old_state.shape, F32),
        ),
        in_specs=[vmem, vmem, anywhere],
        out_specs=(anywhere, anywhere),
        scratch_shapes=[
            pltpu.VMEM((1, width), F32),
            pltpu.VMEM((rows, width), F32),
            pltpu.VMEM((rows, half), BF),
            pltpu.SemaphoreType.DMA((6,)),
        ],
    )(
        pltpu.with_memory_space_constraint(total, pltpu.VMEM),
        pltpu.with_memory_space_constraint(new_state, pltpu.VMEM),
        moe_gain.reshape(1, width),
    )


def solution(mesh):
    in_specs = (
        P("ep", None),
        P("ep", "tp", None),
        P(None, "tp"),
        P(None, "tp"),
        P(None, "tp"),
        P(None, "tp"),
        P("tp"),
        P(),
        P("tp", None),
        P(),
        P("ep", None, "tp"),
        P("ep", None, "tp"),
        P("ep", "tp", None),
        P("ep", None),
        P("ep", None),
        P(),
    )
    out_specs = (P("ep", "tp"), P("ep", "tp", None))
    return jax.shard_map(
        per_device, mesh=mesh, in_specs=in_specs, out_specs=out_specs, check_vma=False
    )
```

```python
import jax
import jax.numpy as jnp
from jax import lax
from jax.experimental import pallas as pl
from jax.experimental.pallas import tpu as pltpu
from jax.sharding import PartitionSpec as P

MESH = pl.DeviceIdType.MESH
BF = jnp.bfloat16
F32 = jnp.float32


def dot(a, b):
    return jnp.dot(a, b, preferred_element_type=F32)


def silu(v):
    return v / (1.0 + jnp.exp(-v))


AXES = (8, 4, 4)
CHIPS = AXES[1] * AXES[2]
PLANE = CHIPS // 2
FAR = ((4,),)
Z_ORDER = (3, 5, 2, 6, 1, 7, 0)
GROUPS = ((0, 2), (2, 4), (4, 7))
HOME = Z_ORDER.index(0)
SELF = HOME * PLANE
RING = AXES[2]
WIDE = 4


def kernel(
    tokens,
    old,
    w_query,
    w_forget,
    w_value,
    w_gate,
    bound_in,
    head_gain_in,
    w_out,
    mix_gain_in,
    e_gate,
    e_up,
    e_down,
    ids_in,
    weight_in,
    total_out,
    st,
    tok,
    wq,
    wf,
    wv,
    wg,
    wo,
    eg,
    eu,
    ed,
    eg_far,
    eu_far,
    ed_far,
    bound,
    head_gain,
    mix_gain,
    ids,
    weight,
    f_s,
    q_s,
    v_s,
    r_s,
    gates,
    mix,
    own_part,
    other_part,
    after,
    send,
    recv,
    ret_send,
    ret_recv,
    far_refs,
    own_moe,
    other_moe,
    small,
    in_sem,
    tp_send,
    tp_recv,
    ep_send,
    ep_recv,
    far_send_sem,
    far_recv_sem,
):
    me = lax.axis_index("ep")
    core = lax.axis_index("tp")
    rows, width = tok.shape
    heads = st.shape[1]
    blocks = width // 128
    slots = len(Z_ORDER) * PLANE
    n_keys = st.shape[2]
    my_z = lax.div(me, CHIPS)
    my_y = lax.rem(lax.div(me, AXES[2]), AXES[1])
    my_x = lax.rem(me, AXES[2])
    z_at = [lax.rem(my_z + dz, AXES[0]) * CHIPS for dz in range(AXES[0])]
    x_at = {
        (sign, q): lax.rem(my_x + AXES[2] + sign * (2 * q + core), AXES[2])
        for sign in (1, -1)
        for q in (0, 1)
    }

    def far_peers(g, sign):
        for i, dz in enumerate(FAR[g]):
            for h in range(2):
                y = lax.rem(my_y + AXES[1] + sign * (2 * h + core), AXES[1])
                yield 2 * i + h, z_at[(sign * dz) % AXES[0]] + y * AXES[2] + my_x

    def ring_peer(dx):
        return me - my_x + lax.rem(my_x + AXES[2] + dx, AXES[2])

    def each_of_plane(pos, sign, visit):
        dz = Z_ORDER[pos]
        base = z_at[(sign * dz) % AXES[0]]

        def one(dy, q):
            y = my_y + dy if sign > 0 else my_y + AXES[1] - dy
            y = jnp.where(y >= AXES[1], y - AXES[1], y) * AXES[2]
            visit(pos * PLANE + dy * 2 + q, base + y + x_at[sign, q])

        def body(dy, carry):
            one(dy, 0)
            one(dy, 1)
            return carry

        if dz == 0:

            @pl.when(core == 1)
            def _():
                one(0, 0)

            one(0, 1)
        lax.fori_loop(1 if dz == 0 else 0, AXES[1], body, 0)

    part = n_keys // 4
    pieces = [
        (tokens, tok),
        (bound_in, bound),
        (w_forget, wf),
        (w_query, wq),
        (w_value, wv),
        *((old.at[:, :, pl.ds(i * part, part)], st.at[:, :, pl.ds(i * part, part)]) for i in range(4)),
        (w_gate, wg),
        (head_gain_in, head_gain),
        (w_out, wo),
        (mix_gain_in, mix_gain),
        (ids_in, ids),
        (weight_in, weight),
        (e_gate.at[0], eg),
        (e_up.at[0], eu),
        (e_down.at[0], ed),
    ]
    loads = [pltpu.make_async_copy(src, dst, in_sem.at[i]) for i, (src, dst) in enumerate(pieces)]
    for load in loads:
        load.start()
    l_tok, l_bound, l_wf, l_wq, l_wv = loads[:5]
    l_state = loads[5:9]
    l_wg, l_hg, l_wo, l_mg, l_ids, l_weight, l_eg, l_eu, l_ed = loads[9:]

    barrier = pltpu.get_barrier_semaphore()
    pl.semaphore_signal(barrier, inc=1, device_id=(me, 1 - core), device_id_type=MESH)

    def greet(slot, peer):
        pl.semaphore_signal(barrier, inc=1, device_id=(peer, core), device_id_type=MESH)

    for g in range(len(FAR)):
        for slot, peer in far_peers(g, 1):
            greet(slot, peer)
    for pos in range(len(Z_ORDER)):
        each_of_plane(pos, 1, greet)
    for dx in range(1, RING):
        greet(dx, ring_peer(dx))

    pairs = heads // 2
    tall = rows * heads

    def by_head(ref, values, p):
        ref[pl.ds(2 * p, rows, heads), :] = values
        ref[pl.ds(2 * p + 1, rows, heads), :] = values

    lane = lax.broadcasted_iota(jnp.int32, (tall, 128), 1)
    head = lax.broadcasted_iota(jnp.int32, (tall, 128), 0)
    mine = lax.shift_right_logical(lane, 6) == lax.bitwise_and(head, 1)

    def split(ref, first):
        values = jnp.where(mine, ref[...], 0.0)
        high = values.astype(BF)
        gates[first : first + tall, 0:128] = high
        gates[first : first + tall, 128:256] = (values - high.astype(F32)).astype(BF)

    l_tok.wait()
    x = tok[...]
    l_bound.wait()
    l_wf.wait()
    f_lin = dot(x, wf[...])
    for p in range(pairs):
        cols = slice(p * 128, (p + 1) * 128)
        low = bound[:, cols]
        by_head(f_s, low + (1.0 - low) / (1.0 + jnp.exp(-f_lin[:, cols])), p)
    split(f_s, 0)
    l_wq.wait()
    q_lin = dot(x, wq[...])
    for p in range(pairs):
        by_head(q_s, silu(q_lin[:, p * 128 : (p + 1) * 128]), p)
    split(q_s, tall)
    l_wv.wait()
    v_lin = dot(x, wv[...])
    for p in range(pairs):
        by_head(v_s, v_lin[:, p * 128 : (p + 1) * 128], p)
    v_pair = v_s[...]
    v_s[...] = jnp.where(mine, v_pair, pltpu.roll(v_pair, 64, 1))
    r_s[...] = jnp.zeros_like(r_s)

    tile = 256
    key_gap = (
        lax.bitwise_and(lax.broadcasted_iota(jnp.int32, (tile, tile), 0), 63)
        - lax.shift_right_logical(lax.broadcasted_iota(jnp.int32, (tile, tile), 1), 6)
    ).astype(F32)

    def one_tile(n):
        spread = jnp.where(key_gap == 4.0 * n, 1.0, 0.0).astype(BF)
        both = dot(gates[...], spread)
        cols = slice(n * tile, (n + 1) * tile)
        previous = st[:, :, cols].reshape(tall, tile)
        value = jnp.concatenate([v_s[...], v_s[...]], axis=1)
        new = value + both[:tall] * (previous - value)
        st[:, :, cols] = new.reshape(rows, heads, tile)
        read = both[tall:] * new
        return read[:, :128] + read[:, 128:]

    per_part = part // tile
    for i in range(4):
        l_state[i].wait()
        for n in range(i * per_part, (i + 1) * per_part):
            r_s[...] += one_tile(n)
    r_s[...] += pltpu.roll(r_s[...], 64, 1)

    l_wg.wait()
    l_hg.wait()
    g_lin = dot(x, wg[...])
    first_head = lax.broadcasted_iota(jnp.int32, (rows, 128), 1) < 64
    gain2 = jnp.concatenate([head_gain[...], head_gain[...]], axis=1)
    for p in range(pairs):
        cols = slice(p * 128, (p + 1) * 128)
        even_head = r_s[pl.ds(2 * p, rows, heads), :]
        odd_head = r_s[pl.ds(2 * p + 1, rows, heads), :]
        even_head = even_head * lax.rsqrt(
            jnp.sum(even_head * even_head, -1, keepdims=True) / 128.0 + 1e-6
        )
        odd_head = odd_head * lax.rsqrt(
            jnp.sum(odd_head * odd_head, -1, keepdims=True) / 128.0 + 1e-6
        )
        normed = jnp.where(first_head, even_head, odd_head) * gain2
        mix[:, cols] = (normed * silu(g_lin[:, cols])).astype(BF)
    l_wo.wait()
    own_part[...] = dot(mix[...], wo[...]).astype(BF)

    n_far = sum(2 * len(group) for group in FAR)
    pl.semaphore_wait(barrier, slots + core + n_far + RING - 1)

    def to_partner(src, dst, i):
        return pltpu.make_async_remote_copy(
            src_ref=src,
            dst_ref=dst,
            send_sem=tp_send.at[i],
            recv_sem=tp_recv.at[i],
            device_id=(me, 1 - core),
            device_id_type=MESH,
        )

    swap = to_partner(own_part, other_part, 0)
    swap.start()

    for load in (l_eg, l_eu, l_ed):
        load.wait()
    halves = [to_partner(eg, eg_far, 1), to_partner(eu, eu_far, 2), to_partner(ed, ed_far, 3)]
    for push in halves:
        push.start()

    for load in (l_ids, l_weight, l_mg):
        load.wait()
    small[...] = jnp.zeros_like(small)
    small[0:2, 0:rows] = ids[...].astype(F32)
    small[2:4, 0:rows] = weight[...]
    turned = small[...].T[0:rows]
    id0 = turned[:, 0:1].astype(jnp.int32)
    id1 = turned[:, 1:2].astype(jnp.int32)
    slot_iota = lax.broadcasted_iota(jnp.int32, (rows, 128), 1)
    slot_pos = lax.shift_right_logical(slot_iota, 4)
    dz = jnp.zeros_like(slot_pos)
    for pos, offset in enumerate(Z_ORDER):
        dz = jnp.where(slot_pos == pos, offset, dz)
    dy = lax.bitwise_and(lax.shift_right_logical(slot_iota, 2), 3)
    dx = lax.bitwise_and(slot_iota, 2) + core
    expert = (
        lax.bitwise_and(my_z + dz, 7) * CHIPS
        + lax.bitwise_and(my_y + dy, 3) * AXES[2]
        + lax.bitwise_and(my_x + dx, 3)
    )
    names0 = expert == id0
    names1 = expert == id1
    named = jnp.where(names0 | names1, 1.0, 0.0)
    r_iota = lax.broadcasted_iota(jnp.int32, (rows, rows), 0)
    c_iota = lax.broadcasted_iota(jnp.int32, (rows, rows), 1)
    earlier = jnp.where(c_iota < r_iota, 1.0, 0.0)
    rank = dot(earlier.astype(BF), named.astype(BF))
    slot_of = lax.bitwise_and(slot_iota, 1).astype(F32)
    takes = jnp.where(rank == slot_of, named, 0.0)
    route = jnp.where(names0, turned[:, 2:3], 0.0) + jnp.where(names1, turned[:, 3:4], 0.0)
    route = jnp.where(rank == slot_of, route, 0.0)
    route_high = route.astype(BF)
    route_low = (route - route_high.astype(F32)).astype(BF)
    route_both = jnp.concatenate([route_high.astype(F32), route_low.astype(F32)], axis=0).astype(BF)
    choose = takes.T.astype(BF)

    ring_of = lax.shift_right_logical(id0, 2)
    far_takes = []
    for group in FAR:
        far_pos = lax.shift_right_logical(slot_iota, 3)
        dz = jnp.zeros_like(far_pos)
        for i, offset in enumerate(group):
            dz = jnp.where(far_pos == i, offset, dz)
        dy = lax.bitwise_and(lax.shift_right_logical(slot_iota, 1), 2) + core
        ring = lax.bitwise_and(my_z + dz, 7) * AXES[1] + lax.bitwise_and(my_y + dy, 3)
        named = jnp.where(ring == ring_of, 1.0, 0.0)
        rank = dot(earlier.astype(BF), named.astype(BF))
        named = jnp.where(rank == lax.bitwise_and(slot_iota, 3).astype(F32), named, 0.0)
        far_takes.append(named)
    far_choose = [named.T.astype(BF) for named in far_takes]
    x_of = lax.bitwise_and(slot_iota, 3)
    ring_weight = jnp.where(x_of == lax.bitwise_and(id0, 3), turned[:, 2:3], 0.0) + jnp.where(
        x_of == lax.bitwise_and(id1, 3), turned[:, 3:4], 0.0
    )
    weight_high = ring_weight.astype(BF)
    weight_low = (ring_weight - weight_high.astype(F32)).astype(BF)
    weight_terms = jnp.where(
        slot_iota < 4, weight_high.astype(F32), jnp.where(slot_iota < 8, weight_low.astype(F32), 0.0)
    ).astype(BF)
    swap.wait()
    mixed = own_part[...].astype(F32) + other_part[...].astype(F32)
    full = x.astype(F32) + mixed
    centered = full - jnp.mean(full, -1, keepdims=True)
    variance = jnp.mean(centered * centered, -1, keepdims=True)
    after[...] = (centered * lax.rsqrt(variance + 1e-5) * mix_gain[...]).astype(BF)

    def exchange(src, dst, send_sem, recv_sem, group, sign):
        def give(slot, peer):
            pltpu.make_async_remote_copy(
                src_ref=src.at[:, slot],
                dst_ref=dst.at[:, slot],
                send_sem=send_sem,
                recv_sem=recv_sem,
                device_id=(peer, core),
                device_id_type=MESH,
            ).start()

        for pos in range(*group):
            each_of_plane(pos, sign, give)
        if group[0] <= HOME < group[1]:

            @pl.when(core == 0)
            def _():
                dst[:, SELF : SELF + 1] = src[:, SELF : SELF + 1]

    def bytes_of(src, dst, send_sem, recv_sem, first, count):
        return pltpu.make_async_remote_copy(
            src_ref=src.at[:, pl.ds(first, count)],
            dst_ref=dst.at[:, pl.ds(first, count)],
            send_sem=send_sem,
            recv_sem=recv_sem,
            device_id=(me, 1 - core),
            device_id_type=MESH,
        )

    def span(group):
        return group[0] * PLANE, group[1] * PLANE

    def arrived(src, dst, send_sem, recv_sem, group):
        first, last = span(group)
        if group[0] <= HOME < group[1]:

            @pl.when(core == 0)
            def _():
                bytes_of(src, dst, send_sem, recv_sem, first, last - first - 1).wait_recv()

            @pl.when(core == 1)
            def _():
                bytes_of(src, dst, send_sem, recv_sem, first, last - first).wait_recv()

        else:
            bytes_of(src, dst, send_sem, recv_sem, first, last - first).wait_recv()

    def put_rows(buf, values, first, last):
        for j in range(blocks):
            buf[j, first:last] = values[:, j * 128 : (j + 1) * 128].reshape(last - first, 2, 128)

    def rows_of(buf, first, last):
        return jnp.concatenate(
            [buf[j, first:last].reshape(2 * (last - first), 128) for j in range(blocks)], axis=1
        )

    def expert(inputs):
        hidden = (silu(dot(inputs, eg[...])) * dot(inputs, eu[...])).astype(BF)
        hidden_far = (silu(dot(inputs, eg_far[...])) * dot(inputs, eu_far[...])).astype(BF)
        result = dot(hidden, ed[...]).astype(BF).astype(F32)
        result_far = dot(hidden_far, ed_far[...]).astype(BF).astype(F32)
        return (result + result_far).astype(BF)

    def far_copy(src, dst, kind, g, peer):
        at = kind * len(FAR) + g
        return pltpu.make_async_remote_copy(
            src_ref=src,
            dst_ref=dst,
            send_sem=far_send_sem.at[at],
            recv_sem=far_recv_sem.at[at],
            device_id=(peer, core),
            device_id_type=MESH,
        )

    def far_dispatch(g):
        out, arrive = far_refs[g][0:2]
        n = out.shape[1]
        picked = dot(far_choose[g][: WIDE * n], after[...]).astype(BF)
        for j in range(blocks):
            out[j] = picked[:, j * 128 : (j + 1) * 128].reshape(n, WIDE, 128)
        out[blocks] = dot(far_choose[g][: WIDE * n], weight_terms).astype(BF).reshape(n, WIDE, 128)
        for slot, peer in far_peers(g, 1):
            far_copy(out.at[:, slot], arrive.at[:, slot], 0, g, peer).start()

    def far_hand_round(g):
        out, arrive, ring_in = far_refs[g][0:3]
        far_copy(out, arrive, 0, g, ring_peer(1)).wait_recv()
        for dx in range(1, RING):
            far_copy(arrive, ring_in.at[:, dx], 1, g, ring_peer(dx)).start()
        ring_in[:, 0] = arrive[...]

    def far_expert(g):
        ring_in, back, back_in = far_refs[g][2:5]
        n = ring_in.shape[2]
        count = RING * n * WIDE
        rest = pl.ds(1, RING - 1)
        far_copy(ring_in.at[:, rest], ring_in.at[:, rest], 1, g, ring_peer(1)).wait_recv()
        inputs = jnp.concatenate(
            [ring_in[j].reshape(count, 128) for j in range(blocks)], axis=1
        )
        terms = ring_in[blocks].reshape(count, 128).astype(F32)
        at = lax.broadcasted_iota(jnp.int32, (count, 128), 1)
        mine = lax.bitwise_and(at, 3) == my_x
        scale = jnp.sum(jnp.where(mine, terms, 0.0), -1, keepdims=True)
        given = (expert(inputs).astype(F32) * scale).astype(BF)
        for j in range(blocks):
            back[j] = given[:, j * 128 : (j + 1) * 128].reshape(RING, n, WIDE, 128)
        for dx in range(1, RING):
            far_copy(back.at[:, dx], back_in.at[:, dx], 2, g, ring_peer(-dx)).start()
        back_in[:, 0] = back[:, 0]

    def far_sum(g):
        back_in, out, home = far_refs[g][4:7]
        n = out.shape[1]
        rest = pl.ds(1, RING - 1)
        far_copy(back_in.at[:, rest], back_in.at[:, rest], 2, g, ring_peer(1)).wait_recv()
        for j in range(blocks):
            parts = back_in[j].reshape(RING * n * WIDE, 128).astype(F32).reshape(RING, n * WIDE, 128)
            out[j] = jnp.sum(parts, axis=0).astype(BF).reshape(n, WIDE, 128)
        for slot, peer in far_peers(g, -1):
            far_copy(out.at[:, slot], home.at[:, slot], 3, g, peer).start()

    for g in range(len(FAR)):
        far_dispatch(g)
    def near_dispatch(g):
        first, last = span(GROUPS[g])
        put_rows(send, dot(choose[2 * first : 2 * last], after[...]).astype(BF), first, last)
        exchange(send, recv, ep_send.at[0], ep_recv.at[g], GROUPS[g], 1)

    def near_expert(g):
        group = GROUPS[g]
        first, last = span(group)
        arrived(send, recv, ep_send.at[0], ep_recv.at[g], group)
        put_rows(ret_send, expert(rows_of(recv, first, last)), first, last)
        exchange(ret_send, ret_recv, ep_send.at[1], ep_recv.at[len(GROUPS) + g], group, -1)

    near_dispatch(0)
    far_hand_round(0)
    near_dispatch(1)
    near_dispatch(2)
    for push in halves:
        push.wait_recv()
    near_expert(0)
    far_expert(0)
    near_expert(1)
    far_sum(0)
    near_expert(2)

    moe_sum = None
    for g, group in enumerate(GROUPS):
        first, last = span(group)
        arrived(ret_send, ret_recv, ep_send.at[1], ep_recv.at[len(GROUPS) + g], group)
        both = dot(route_both[:, 2 * first : 2 * last], rows_of(ret_recv, first, last))
        both = both[:rows] + both[rows:]
        moe_sum = both if moe_sum is None else moe_sum + both
    for g in range(len(FAR)):
        out, home = far_refs[g][5:7]
        n = home.shape[1]
        far_copy(out, home, 3, g, ring_peer(1)).wait_recv()
        rows_back = jnp.concatenate(
            [home[j].reshape(n * WIDE, 128) for j in range(blocks)], axis=1
        )
        moe_sum = moe_sum + dot(far_takes[g][:, : n * WIDE].astype(BF), rows_back)
    own_moe[...] = moe_sum
    last_swap = to_partner(own_moe, other_moe, 4)
    last_swap.start()
    @pl.when(core == 0)
    def _():
        bytes_of(send, recv, ep_send.at[0], ep_recv.at[0], 0, slots - 1).wait_send()
        bytes_of(ret_send, ret_recv, ep_send.at[1], ep_recv.at[0], 0, slots - 1).wait_send()

    @pl.when(core == 1)
    def _():
        bytes_of(send, recv, ep_send.at[0], ep_recv.at[0], 0, slots).wait_send()
        bytes_of(ret_send, ret_recv, ep_send.at[1], ep_recv.at[0], 0, slots).wait_send()

    for g in range(len(FAR)):
        out, arrive, ring_in, back, back_in, total, home = far_refs[g]
        rest = pl.ds(1, RING - 1)
        far_copy(out, arrive, 0, g, ring_peer(1)).wait_send()
        far_copy(ring_in.at[:, rest], ring_in.at[:, rest], 1, g, ring_peer(1)).wait_send()
        far_copy(back.at[:, rest], back_in.at[:, rest], 2, g, ring_peer(1)).wait_send()
        far_copy(total, home, 3, g, ring_peer(1)).wait_send()
    for remote in halves:
        remote.wait_send()
    last_swap.wait_recv()
    total_out[...] = after[...].astype(F32) + (own_moe[...] + other_moe[...])
    last_swap.wait_send()


def finish(total, state_in, moe_gain_in, next_out, state_out, moe_gain, normed, result, sem):
    core = lax.axis_index("tp")
    half = next_out.shape[1]
    parts = sem.shape[0] - 2
    rows = state_in.shape[0] // parts
    gain_load = pltpu.make_async_copy(moe_gain_in, moe_gain, sem.at[parts])
    gain_load.start()
    copies = [
        pltpu.make_async_copy(
            state_in.at[pl.ds(i * rows, rows)], state_out.at[pl.ds(i * rows, rows)], sem.at[i]
        )
        for i in range(parts)
    ]
    for copy in copies:
        copy.start()
    values = total[...]
    centered = values - jnp.mean(values, -1, keepdims=True)
    scale = lax.rsqrt(jnp.mean(centered * centered, -1, keepdims=True) + 1e-5)
    gain_load.wait()
    normed[...] = centered * scale * moe_gain[...]
    result[...] = normed[:, pl.ds(pl.multiple_of(core * half, 128), half)].astype(BF)
    copies.append(pltpu.make_async_copy(result, next_out, sem.at[parts + 1]))
    copies[-1].start()
    for copy in copies:
        copy.wait()


def per_device(
    tokens,
    old_state,
    w_query,
    w_forget,
    w_value,
    w_gate,
    lower_bound,
    head_gain,
    w_out,
    mix_gain,
    expert_gate,
    expert_up,
    expert_down,
    expert_ids,
    route_weight,
    moe_gain,
):
    rows, width = tokens.shape
    heads = old_state.shape[1]
    cols = w_query.shape[1]
    units = expert_gate.shape[2]
    half = width // 2
    tall = rows * heads
    anywhere = pl.BlockSpec(memory_space=pl.ANY)
    vmem = pl.BlockSpec(memory_space=pltpu.VMEM)
    blocks = width // 128
    message = pltpu.VMEM((blocks, len(Z_ORDER) * PLANE, 2, 128), BF)
    far = tuple(
        (
            pltpu.VMEM((blocks + 1, 2 * len(group), WIDE, 128), BF),
            pltpu.VMEM((blocks + 1, 2 * len(group), WIDE, 128), BF),
            pltpu.VMEM((blocks + 1, RING, 2 * len(group), WIDE, 128), BF),
            pltpu.VMEM((blocks, RING, 2 * len(group), WIDE, 128), BF),
            pltpu.VMEM((blocks, RING, 2 * len(group), WIDE, 128), BF),
            pltpu.VMEM((blocks, 2 * len(group), WIDE, 128), BF),
            pltpu.VMEM((blocks, 2 * len(group), WIDE, 128), BF),
        )
        for group in FAR
    )
    by_head = pltpu.VMEM((tall, 128), F32)
    row = pltpu.VMEM((rows, width), BF)
    total, new_state = pl.pallas_call(
        kernel,
        out_shape=(
            pltpu.VMEM((rows, width), F32),
            pltpu.VMEM(old_state.shape, F32),
        ),
        in_specs=[anywhere] * 15,
        out_specs=(vmem, vmem),
        scratch_shapes=[
            row,
            *[pltpu.VMEM((width, cols), BF)] * 4,
            pltpu.VMEM((cols, width), BF),
            *[pltpu.VMEM((width, units), BF), pltpu.VMEM((width, units), BF), pltpu.VMEM((units, width), BF)] * 2,
            pltpu.VMEM((1, cols), F32),
            pltpu.VMEM((1, head_gain.shape[0]), F32),
            pltpu.VMEM((1, width), F32),
            pltpu.VMEM((2, rows), jnp.int32),
            pltpu.VMEM((2, rows), F32),
            by_head,
            by_head,
            by_head,
            by_head,
            pltpu.VMEM((2 * tall, 256), BF),
            pltpu.VMEM((rows, cols), BF),
            row,
            row,
            row,
            message,
            message,
            message,
            message,
            far,
            pltpu.VMEM((rows, width), F32),
            pltpu.VMEM((rows, width), F32),
            pltpu.VMEM((8, 128), F32),
            pltpu.SemaphoreType.DMA((18,)),
            pltpu.SemaphoreType.DMA((5,)),
            pltpu.SemaphoreType.DMA((5,)),
            pltpu.SemaphoreType.DMA((2,)),
            pltpu.SemaphoreType.DMA((2 * len(GROUPS),)),
            pltpu.SemaphoreType.DMA((4 * len(FAR),)),
            pltpu.SemaphoreType.DMA((4 * len(FAR),)),
        ],
        compiler_params=pltpu.CompilerParams(
            collective_id=0, has_side_effects=True, vmem_limit_bytes=56 * 1024 * 1024
        ),
    )(
        tokens,
        old_state,
        w_query,
        w_forget,
        w_value,
        w_gate,
        lower_bound.reshape(1, cols),
        head_gain.reshape(1, -1),
        w_out,
        mix_gain.reshape(1, width),
        expert_gate,
        expert_up,
        expert_down,
        expert_ids.T,
        route_weight.T,
    )
    return pl.pallas_call(
        finish,
        out_shape=(
            jax.ShapeDtypeStruct((rows, half), BF),
            jax.ShapeDtypeStruct(old_state.shape, F32),
        ),
        in_specs=[vmem, vmem, anywhere],
        out_specs=(anywhere, anywhere),
        scratch_shapes=[
            pltpu.VMEM((1, width), F32),
            pltpu.VMEM((rows, width), F32),
            pltpu.VMEM((rows, half), BF),
            pltpu.SemaphoreType.DMA((6,)),
        ],
    )(
        pltpu.with_memory_space_constraint(total, pltpu.VMEM),
        pltpu.with_memory_space_constraint(new_state, pltpu.VMEM),
        moe_gain.reshape(1, width),
    )


def solution(mesh):
    in_specs = (
        P("ep", None),
        P("ep", "tp", None),
        P(None, "tp"),
        P(None, "tp"),
        P(None, "tp"),
        P(None, "tp"),
        P("tp"),
        P(),
        P("tp", None),
        P(),
        P("ep", None, "tp"),
        P("ep", None, "tp"),
        P("ep", "tp", None),
        P("ep", None),
        P("ep", None),
        P(),
    )
    out_specs = (P("ep", "tp"), P("ep", "tp", None))
    return jax.shard_map(
        per_device, mesh=mesh, in_specs=in_specs, out_specs=out_specs, check_vma=False
    )
```

```python
import jax
import jax.numpy as jnp
from jax import lax
from jax.experimental import pallas as pl
from jax.experimental.pallas import tpu as pltpu
from jax.sharding import PartitionSpec as P

MESH = pl.DeviceIdType.MESH
BF = jnp.bfloat16
F32 = jnp.float32


def dot(a, b):
    return jnp.dot(a, b, preferred_element_type=F32)


def silu(v):
    return v / (1.0 + jnp.exp(-v))


AXES = (8, 4, 4)
CHIPS = AXES[1] * AXES[2]
PLANE = CHIPS // 2
FAR = ((4,),)
Z_ORDER = (3, 5, 2, 6, 1, 7, 0)
GROUPS = ((0, 2), (2, 4), (4, 7))
HOME = Z_ORDER.index(0)
SELF = HOME * PLANE
RING = AXES[2]
WIDE = 4


def kernel(
    tokens,
    old,
    w_query,
    w_forget,
    w_value,
    w_gate,
    bound_in,
    head_gain_in,
    w_out,
    mix_gain_in,
    e_gate,
    e_up,
    e_down,
    ids_in,
    weight_in,
    total_out,
    st,
    tok,
    wq,
    wf,
    wv,
    wg,
    wo,
    eg,
    eu,
    ed,
    eg_far,
    eu_far,
    ed_far,
    bound,
    head_gain,
    mix_gain,
    ids,
    weight,
    f_s,
    q_s,
    v_s,
    r_s,
    gates,
    mix,
    own_part,
    other_part,
    after,
    send,
    recv,
    ret_send,
    ret_recv,
    far_refs,
    own_moe,
    other_moe,
    small,
    in_sem,
    tp_send,
    tp_recv,
    ep_send,
    ep_recv,
    far_send_sem,
    far_recv_sem,
):
    me = lax.axis_index("ep")
    core = lax.axis_index("tp")
    rows, width = tok.shape
    heads = st.shape[1]
    blocks = width // 128
    slots = len(Z_ORDER) * PLANE
    n_keys = st.shape[2]
    my_z = lax.div(me, CHIPS)
    my_y = lax.rem(lax.div(me, AXES[2]), AXES[1])
    my_x = lax.rem(me, AXES[2])
    z_at = [lax.rem(my_z + dz, AXES[0]) * CHIPS for dz in range(AXES[0])]
    x_at = {
        (sign, q): lax.rem(my_x + AXES[2] + sign * (2 * q + core), AXES[2])
        for sign in (1, -1)
        for q in (0, 1)
    }

    def far_peers(g, sign):
        for i, dz in enumerate(FAR[g]):
            for h in range(2):
                y = lax.rem(my_y + AXES[1] + sign * (2 * h + core), AXES[1])
                yield 2 * i + h, z_at[(sign * dz) % AXES[0]] + y * AXES[2] + my_x

    def ring_peer(dx):
        return me - my_x + lax.rem(my_x + AXES[2] + dx, AXES[2])

    def each_of_plane(pos, sign, visit):
        dz = Z_ORDER[pos]
        base = z_at[(sign * dz) % AXES[0]]

        def one(dy, q):
            y = my_y + dy if sign > 0 else my_y + AXES[1] - dy
            y = jnp.where(y >= AXES[1], y - AXES[1], y) * AXES[2]
            visit(pos * PLANE + dy * 2 + q, base + y + x_at[sign, q])

        def body(dy, carry):
            one(dy, 0)
            one(dy, 1)
            return carry

        if dz == 0:

            @pl.when(core == 1)
            def _():
                one(0, 0)

            one(0, 1)
        lax.fori_loop(1 if dz == 0 else 0, AXES[1], body, 0)

    part = n_keys // 4
    pieces = [
        (tokens, tok),
        (bound_in, bound),
        (w_forget, wf),
        (w_query, wq),
        (w_value, wv),
        *((old.at[:, :, pl.ds(i * part, part)], st.at[:, :, pl.ds(i * part, part)]) for i in range(4)),
        (w_gate, wg),
        (head_gain_in, head_gain),
        (w_out, wo),
        (mix_gain_in, mix_gain),
        (ids_in, ids),
        (weight_in, weight),
        (e_gate.at[0], eg),
        (e_up.at[0], eu),
        (e_down.at[0], ed),
    ]
    loads = [pltpu.make_async_copy(src, dst, in_sem.at[i]) for i, (src, dst) in enumerate(pieces)]
    for load in loads:
        load.start()
    l_tok, l_bound, l_wf, l_wq, l_wv = loads[:5]
    l_state = loads[5:9]
    l_wg, l_hg, l_wo, l_mg, l_ids, l_weight, l_eg, l_eu, l_ed = loads[9:]

    barrier = pltpu.get_barrier_semaphore()
    pl.semaphore_signal(barrier, inc=1, device_id=(me, 1 - core), device_id_type=MESH)

    def greet(slot, peer):
        pl.semaphore_signal(barrier, inc=1, device_id=(peer, core), device_id_type=MESH)

    for g in range(len(FAR)):
        for slot, peer in far_peers(g, 1):
            greet(slot, peer)
    for pos in range(len(Z_ORDER)):
        each_of_plane(pos, 1, greet)
    for dx in range(1, RING):
        greet(dx, ring_peer(dx))

    pairs = heads // 2
    tall = rows * heads

    def by_head(ref, values, p):
        ref[pl.ds(2 * p, rows, heads), :] = values
        ref[pl.ds(2 * p + 1, rows, heads), :] = values

    lane = lax.broadcasted_iota(jnp.int32, (tall, 128), 1)
    head = lax.broadcasted_iota(jnp.int32, (tall, 128), 0)
    mine = lax.shift_right_logical(lane, 6) == lax.bitwise_and(head, 1)

    def split(ref, first):
        values = jnp.where(mine, ref[...], 0.0)
        high = values.astype(BF)
        gates[first : first + tall, 0:128] = high
        gates[first : first + tall, 128:256] = (values - high.astype(F32)).astype(BF)

    l_tok.wait()
    x = tok[...]
    l_bound.wait()
    l_wf.wait()
    f_lin = dot(x, wf[...])
    for p in range(pairs):
        cols = slice(p * 128, (p + 1) * 128)
        low = bound[:, cols]
        by_head(f_s, low + (1.0 - low) / (1.0 + jnp.exp(-f_lin[:, cols])), p)
    split(f_s, 0)
    l_wq.wait()
    q_lin = dot(x, wq[...])
    for p in range(pairs):
        by_head(q_s, silu(q_lin[:, p * 128 : (p + 1) * 128]), p)
    split(q_s, tall)
    l_wv.wait()
    v_lin = dot(x, wv[...])
    for p in range(pairs):
        by_head(v_s, v_lin[:, p * 128 : (p + 1) * 128], p)
    v_pair = v_s[...]
    v_s[...] = jnp.where(mine, v_pair, pltpu.roll(v_pair, 64, 1))
    r_s[...] = jnp.zeros_like(r_s)

    tile = 256
    key_gap = (
        lax.bitwise_and(lax.broadcasted_iota(jnp.int32, (tile, tile), 0), 63)
        - lax.shift_right_logical(lax.broadcasted_iota(jnp.int32, (tile, tile), 1), 6)
    ).astype(F32)

    def one_tile(n):
        spread = jnp.where(key_gap == 4.0 * n, 1.0, 0.0).astype(BF)
        both = dot(gates[...], spread)
        cols = slice(n * tile, (n + 1) * tile)
        previous = st[:, :, cols].reshape(tall, tile)
        value = jnp.concatenate([v_s[...], v_s[...]], axis=1)
        new = value + both[:tall] * (previous - value)
        st[:, :, cols] = new.reshape(rows, heads, tile)
        read = both[tall:] * new
        return read[:, :128] + read[:, 128:]

    per_part = part // tile
    for i in range(4):
        l_state[i].wait()
        for n in range(i * per_part, (i + 1) * per_part):
            r_s[...] += one_tile(n)
    r_s[...] += pltpu.roll(r_s[...], 64, 1)

    l_wg.wait()
    l_hg.wait()
    g_lin = dot(x, wg[...])
    first_head = lax.broadcasted_iota(jnp.int32, (rows, 128), 1) < 64
    gain2 = jnp.concatenate([head_gain[...], head_gain[...]], axis=1)
    for p in range(pairs):
        cols = slice(p * 128, (p + 1) * 128)
        even_head = r_s[pl.ds(2 * p, rows, heads), :]
        odd_head = r_s[pl.ds(2 * p + 1, rows, heads), :]
        even_head = even_head * lax.rsqrt(
            jnp.sum(even_head * even_head, -1, keepdims=True) / 128.0 + 1e-6
        )
        odd_head = odd_head * lax.rsqrt(
            jnp.sum(odd_head * odd_head, -1, keepdims=True) / 128.0 + 1e-6
        )
        normed = jnp.where(first_head, even_head, odd_head) * gain2
        mix[:, cols] = (normed * silu(g_lin[:, cols])).astype(BF)
    l_wo.wait()
    own_part[...] = dot(mix[...], wo[...]).astype(BF)

    n_far = sum(2 * len(group) for group in FAR)
    pl.semaphore_wait(barrier, slots + core + n_far + RING - 1)

    def to_partner(src, dst, i):
        return pltpu.make_async_remote_copy(
            src_ref=src,
            dst_ref=dst,
            send_sem=tp_send.at[i],
            recv_sem=tp_recv.at[i],
            device_id=(me, 1 - core),
            device_id_type=MESH,
        )

    swap = to_partner(own_part, other_part, 0)
    swap.start()

    for load in (l_eg, l_eu, l_ed):
        load.wait()
    halves = [to_partner(eg, eg_far, 1), to_partner(eu, eu_far, 2), to_partner(ed, ed_far, 3)]
    for push in halves:
        push.start()

    for load in (l_ids, l_weight, l_mg):
        load.wait()
    small[...] = jnp.zeros_like(small)
    small[0:2, 0:rows] = ids[...].astype(F32)
    small[2:4, 0:rows] = weight[...]
    turned = small[...].T[0:rows]
    id0 = turned[:, 0:1].astype(jnp.int32)
    id1 = turned[:, 1:2].astype(jnp.int32)
    slot_iota = lax.broadcasted_iota(jnp.int32, (rows, 128), 1)
    slot_pos = lax.shift_right_logical(slot_iota, 4)
    dz = jnp.zeros_like(slot_pos)
    for pos, offset in enumerate(Z_ORDER):
        dz = jnp.where(slot_pos == pos, offset, dz)
    dy = lax.bitwise_and(lax.shift_right_logical(slot_iota, 2), 3)
    dx = lax.bitwise_and(slot_iota, 2) + core
    expert = (
        lax.bitwise_and(my_z + dz, 7) * CHIPS
        + lax.bitwise_and(my_y + dy, 3) * AXES[2]
        + lax.bitwise_and(my_x + dx, 3)
    )
    names0 = expert == id0
    names1 = expert == id1
    named = jnp.where(names0 | names1, 1.0, 0.0)
    r_iota = lax.broadcasted_iota(jnp.int32, (rows, rows), 0)
    c_iota = lax.broadcasted_iota(jnp.int32, (rows, rows), 1)
    earlier = jnp.where(c_iota < r_iota, 1.0, 0.0)
    rank = dot(earlier.astype(BF), named.astype(BF))
    slot_of = lax.bitwise_and(slot_iota, 1).astype(F32)
    takes = jnp.where(rank == slot_of, named, 0.0)
    route = jnp.where(names0, turned[:, 2:3], 0.0) + jnp.where(names1, turned[:, 3:4], 0.0)
    route = jnp.where(rank == slot_of, route, 0.0)
    route_high = route.astype(BF)
    route_low = (route - route_high.astype(F32)).astype(BF)
    route_both = jnp.concatenate([route_high.astype(F32), route_low.astype(F32)], axis=0).astype(BF)
    choose = takes.T.astype(BF)

    ring_of = lax.shift_right_logical(id0, 2)
    far_takes = []
    for group in FAR:
        far_pos = lax.shift_right_logical(slot_iota, 3)
        dz = jnp.zeros_like(far_pos)
        for i, offset in enumerate(group):
            dz = jnp.where(far_pos == i, offset, dz)
        dy = lax.bitwise_and(lax.shift_right_logical(slot_iota, 1), 2) + core
        ring = lax.bitwise_and(my_z + dz, 7) * AXES[1] + lax.bitwise_and(my_y + dy, 3)
        named = jnp.where(ring == ring_of, 1.0, 0.0)
        rank = dot(earlier.astype(BF), named.astype(BF))
        named = jnp.where(rank == lax.bitwise_and(slot_iota, 3).astype(F32), named, 0.0)
        far_takes.append(named)
    far_choose = [named.T.astype(BF) for named in far_takes]
    x_of = lax.bitwise_and(slot_iota, 3)
    ring_weight = jnp.where(x_of == lax.bitwise_and(id0, 3), turned[:, 2:3], 0.0) + jnp.where(
        x_of == lax.bitwise_and(id1, 3), turned[:, 3:4], 0.0
    )
    weight_high = ring_weight.astype(BF)
    weight_low = (ring_weight - weight_high.astype(F32)).astype(BF)
    weight_terms = jnp.where(
        slot_iota < 4, weight_high.astype(F32), jnp.where(slot_iota < 8, weight_low.astype(F32), 0.0)
    ).astype(BF)
    swap.wait()
    mixed = own_part[...].astype(F32) + other_part[...].astype(F32)
    full = x.astype(F32) + mixed
    centered = full - jnp.mean(full, -1, keepdims=True)
    variance = jnp.mean(centered * centered, -1, keepdims=True)
    after[...] = (centered * lax.rsqrt(variance + 1e-5) * mix_gain[...]).astype(BF)

    def exchange(src, dst, send_sem, recv_sem, group, sign):
        def give(slot, peer):
            pltpu.make_async_remote_copy(
                src_ref=src.at[:, slot],
                dst_ref=dst.at[:, slot],
                send_sem=send_sem,
                recv_sem=recv_sem,
                device_id=(peer, core),
                device_id_type=MESH,
            ).start()

        for pos in range(*group):
            each_of_plane(pos, sign, give)
        if group[0] <= HOME < group[1]:

            @pl.when(core == 0)
            def _():
                dst[:, SELF : SELF + 1] = src[:, SELF : SELF + 1]

    def bytes_of(src, dst, send_sem, recv_sem, first, count):
        return pltpu.make_async_remote_copy(
            src_ref=src.at[:, pl.ds(first, count)],
            dst_ref=dst.at[:, pl.ds(first, count)],
            send_sem=send_sem,
            recv_sem=recv_sem,
            device_id=(me, 1 - core),
            device_id_type=MESH,
        )

    def span(group):
        return group[0] * PLANE, group[1] * PLANE

    def arrived(src, dst, send_sem, recv_sem, group):
        first, last = span(group)
        if group[0] <= HOME < group[1]:

            @pl.when(core == 0)
            def _():
                bytes_of(src, dst, send_sem, recv_sem, first, last - first - 1).wait_recv()

            @pl.when(core == 1)
            def _():
                bytes_of(src, dst, send_sem, recv_sem, first, last - first).wait_recv()

        else:
            bytes_of(src, dst, send_sem, recv_sem, first, last - first).wait_recv()

    def put_rows(buf, values, first, last):
        for j in range(blocks):
            buf[j, first:last] = values[:, j * 128 : (j + 1) * 128].reshape(last - first, 2, 128)

    def rows_of(buf, first, last):
        return jnp.concatenate(
            [buf[j, first:last].reshape(2 * (last - first), 128) for j in range(blocks)], axis=1
        )

    def expert(inputs):
        hidden = (silu(dot(inputs, eg[...])) * dot(inputs, eu[...])).astype(BF)
        hidden_far = (silu(dot(inputs, eg_far[...])) * dot(inputs, eu_far[...])).astype(BF)
        result = dot(hidden, ed[...]).astype(BF).astype(F32)
        result_far = dot(hidden_far, ed_far[...]).astype(BF).astype(F32)
        return (result + result_far).astype(BF)

    def far_copy(src, dst, kind, g, peer):
        at = kind * len(FAR) + g
        return pltpu.make_async_remote_copy(
            src_ref=src,
            dst_ref=dst,
            send_sem=far_send_sem.at[at],
            recv_sem=far_recv_sem.at[at],
            device_id=(peer, core),
            device_id_type=MESH,
        )

    def far_dispatch(g):
        out, arrive = far_refs[g][0:2]
        n = out.shape[1]
        picked = dot(far_choose[g][: WIDE * n], after[...]).astype(BF)
        for j in range(blocks):
            out[j] = picked[:, j * 128 : (j + 1) * 128].reshape(n, WIDE, 128)
        out[blocks] = dot(far_choose[g][: WIDE * n], weight_terms).astype(BF).reshape(n, WIDE, 128)
        for slot, peer in far_peers(g, 1):
            far_copy(out.at[:, slot], arrive.at[:, slot], 0, g, peer).start()

    def far_hand_round(g):
        out, arrive, ring_in = far_refs[g][0:3]
        far_copy(out, arrive, 0, g, ring_peer(1)).wait_recv()
        for dx in range(1, RING):
            far_copy(arrive, ring_in.at[:, dx], 1, g, ring_peer(dx)).start()
        ring_in[:, 0] = arrive[...]

    def far_expert(g):
        ring_in, back, back_in = far_refs[g][2:5]
        n = ring_in.shape[2]
        count = RING * n * WIDE
        rest = pl.ds(1, RING - 1)
        far_copy(ring_in.at[:, rest], ring_in.at[:, rest], 1, g, ring_peer(1)).wait_recv()
        inputs = jnp.concatenate(
            [ring_in[j].reshape(count, 128) for j in range(blocks)], axis=1
        )
        terms = ring_in[blocks].reshape(count, 128).astype(F32)
        at = lax.broadcasted_iota(jnp.int32, (count, 128), 1)
        mine = lax.bitwise_and(at, 3) == my_x
        scale = jnp.sum(jnp.where(mine, terms, 0.0), -1, keepdims=True)
        given = (expert(inputs).astype(F32) * scale).astype(BF)
        for j in range(blocks):
            back[j] = given[:, j * 128 : (j + 1) * 128].reshape(RING, n, WIDE, 128)
        for dx in range(1, RING):
            far_copy(back.at[:, dx], back_in.at[:, dx], 2, g, ring_peer(-dx)).start()
        back_in[:, 0] = back[:, 0]

    def far_sum(g):
        back_in, out, home = far_refs[g][4:7]
        n = out.shape[1]
        rest = pl.ds(1, RING - 1)
        far_copy(back_in.at[:, rest], back_in.at[:, rest], 2, g, ring_peer(1)).wait_recv()
        for j in range(blocks):
            parts = back_in[j].reshape(RING * n * WIDE, 128).astype(F32).reshape(RING, n * WIDE, 128)
            out[j] = jnp.sum(parts, axis=0).astype(BF).reshape(n, WIDE, 128)
        for slot, peer in far_peers(g, -1):
            far_copy(out.at[:, slot], home.at[:, slot], 3, g, peer).start()

    for g in range(len(FAR)):
        far_dispatch(g)
    def near_dispatch(g):
        first, last = span(GROUPS[g])
        put_rows(send, dot(choose[2 * first : 2 * last], after[...]).astype(BF), first, last)
        exchange(send, recv, ep_send.at[0], ep_recv.at[g], GROUPS[g], 1)

    def near_expert(g):
        group = GROUPS[g]
        first, last = span(group)
        arrived(send, recv, ep_send.at[0], ep_recv.at[g], group)
        put_rows(ret_send, expert(rows_of(recv, first, last)), first, last)
        exchange(ret_send, ret_recv, ep_send.at[1], ep_recv.at[len(GROUPS) + g], group, -1)

    near_dispatch(0)
    far_hand_round(0)
    near_dispatch(1)
    near_dispatch(2)
    for push in halves:
        push.wait_recv()
    near_expert(0)
    far_expert(0)
    near_expert(1)
    far_sum(0)
    near_expert(2)

    moe_sum = None
    for g, group in enumerate(GROUPS):
        first, last = span(group)
        arrived(ret_send, ret_recv, ep_send.at[1], ep_recv.at[len(GROUPS) + g], group)
        both = dot(route_both[:, 2 * first : 2 * last], rows_of(ret_recv, first, last))
        both = both[:rows] + both[rows:]
        moe_sum = both if moe_sum is None else moe_sum + both
    for g in range(len(FAR)):
        out, home = far_refs[g][5:7]
        n = home.shape[1]
        far_copy(out, home, 3, g, ring_peer(1)).wait_recv()
        rows_back = jnp.concatenate(
            [home[j].reshape(n * WIDE, 128) for j in range(blocks)], axis=1
        )
        moe_sum = moe_sum + dot(far_takes[g][:, : n * WIDE].astype(BF), rows_back)
    own_moe[...] = moe_sum.astype(BF)
    last_swap = to_partner(own_moe, other_moe, 4)
    last_swap.start()
    total_out[...] = after[...].astype(F32) + moe_sum
    @pl.when(core == 0)
    def _():
        bytes_of(send, recv, ep_send.at[0], ep_recv.at[0], 0, slots - 1).wait_send()
        bytes_of(ret_send, ret_recv, ep_send.at[1], ep_recv.at[0], 0, slots - 1).wait_send()

    @pl.when(core == 1)
    def _():
        bytes_of(send, recv, ep_send.at[0], ep_recv.at[0], 0, slots).wait_send()
        bytes_of(ret_send, ret_recv, ep_send.at[1], ep_recv.at[0], 0, slots).wait_send()

    for g in range(len(FAR)):
        out, arrive, ring_in, back, back_in, total, home = far_refs[g]
        rest = pl.ds(1, RING - 1)
        far_copy(out, arrive, 0, g, ring_peer(1)).wait_send()
        far_copy(ring_in.at[:, rest], ring_in.at[:, rest], 1, g, ring_peer(1)).wait_send()
        far_copy(back.at[:, rest], back_in.at[:, rest], 2, g, ring_peer(1)).wait_send()
        far_copy(total, home, 3, g, ring_peer(1)).wait_send()
    for remote in halves:
        remote.wait_send()
    last_swap.wait_recv()
    total_out[...] += other_moe[...].astype(F32)
    last_swap.wait_send()


def finish(total, state_in, moe_gain_in, next_out, state_out, moe_gain, normed, result, sem):
    core = lax.axis_index("tp")
    half = next_out.shape[1]
    parts = sem.shape[0] - 2
    rows = state_in.shape[0] // parts
    gain_load = pltpu.make_async_copy(moe_gain_in, moe_gain, sem.at[parts])
    gain_load.start()
    copies = [
        pltpu.make_async_copy(
            state_in.at[pl.ds(i * rows, rows)], state_out.at[pl.ds(i * rows, rows)], sem.at[i]
        )
        for i in range(parts)
    ]
    for copy in copies:
        copy.start()
    values = total[...]
    centered = values - jnp.mean(values, -1, keepdims=True)
    scale = lax.rsqrt(jnp.mean(centered * centered, -1, keepdims=True) + 1e-5)
    gain_load.wait()
    normed[...] = centered * scale * moe_gain[...]
    result[...] = normed[:, pl.ds(pl.multiple_of(core * half, 128), half)].astype(BF)
    copies.append(pltpu.make_async_copy(result, next_out, sem.at[parts + 1]))
    copies[-1].start()
    for copy in copies:
        copy.wait()


def per_device(
    tokens,
    old_state,
    w_query,
    w_forget,
    w_value,
    w_gate,
    lower_bound,
    head_gain,
    w_out,
    mix_gain,
    expert_gate,
    expert_up,
    expert_down,
    expert_ids,
    route_weight,
    moe_gain,
):
    rows, width = tokens.shape
    heads = old_state.shape[1]
    cols = w_query.shape[1]
    units = expert_gate.shape[2]
    half = width // 2
    tall = rows * heads
    anywhere = pl.BlockSpec(memory_space=pl.ANY)
    vmem = pl.BlockSpec(memory_space=pltpu.VMEM)
    blocks = width // 128
    message = pltpu.VMEM((blocks, len(Z_ORDER) * PLANE, 2, 128), BF)
    far = tuple(
        (
            pltpu.VMEM((blocks + 1, 2 * len(group), WIDE, 128), BF),
            pltpu.VMEM((blocks + 1, 2 * len(group), WIDE, 128), BF),
            pltpu.VMEM((blocks + 1, RING, 2 * len(group), WIDE, 128), BF),
            pltpu.VMEM((blocks, RING, 2 * len(group), WIDE, 128), BF),
            pltpu.VMEM((blocks, RING, 2 * len(group), WIDE, 128), BF),
            pltpu.VMEM((blocks, 2 * len(group), WIDE, 128), BF),
            pltpu.VMEM((blocks, 2 * len(group), WIDE, 128), BF),
        )
        for group in FAR
    )
    by_head = pltpu.VMEM((tall, 128), F32)
    row = pltpu.VMEM((rows, width), BF)
    total, new_state = pl.pallas_call(
        kernel,
        out_shape=(
            pltpu.VMEM((rows, width), F32),
            pltpu.VMEM(old_state.shape, F32),
        ),
        in_specs=[anywhere] * 15,
        out_specs=(vmem, vmem),
        scratch_shapes=[
            row,
            *[pltpu.VMEM((width, cols), BF)] * 4,
            pltpu.VMEM((cols, width), BF),
            *[pltpu.VMEM((width, units), BF), pltpu.VMEM((width, units), BF), pltpu.VMEM((units, width), BF)] * 2,
            pltpu.VMEM((1, cols), F32),
            pltpu.VMEM((1, head_gain.shape[0]), F32),
            pltpu.VMEM((1, width), F32),
            pltpu.VMEM((2, rows), jnp.int32),
            pltpu.VMEM((2, rows), F32),
            by_head,
            by_head,
            by_head,
            by_head,
            pltpu.VMEM((2 * tall, 256), BF),
            pltpu.VMEM((rows, cols), BF),
            row,
            row,
            row,
            message,
            message,
            message,
            message,
            far,
            row,
            row,
            pltpu.VMEM((8, 128), F32),
            pltpu.SemaphoreType.DMA((18,)),
            pltpu.SemaphoreType.DMA((5,)),
            pltpu.SemaphoreType.DMA((5,)),
            pltpu.SemaphoreType.DMA((2,)),
            pltpu.SemaphoreType.DMA((2 * len(GROUPS),)),
            pltpu.SemaphoreType.DMA((4 * len(FAR),)),
            pltpu.SemaphoreType.DMA((4 * len(FAR),)),
        ],
        compiler_params=pltpu.CompilerParams(
            collective_id=0, has_side_effects=True, vmem_limit_bytes=56 * 1024 * 1024
        ),
    )(
        tokens,
        old_state,
        w_query,
        w_forget,
        w_value,
        w_gate,
        lower_bound.reshape(1, cols),
        head_gain.reshape(1, -1),
        w_out,
        mix_gain.reshape(1, width),
        expert_gate,
        expert_up,
        expert_down,
        expert_ids.T,
        route_weight.T,
    )
    return pl.pallas_call(
        finish,
        out_shape=(
            jax.ShapeDtypeStruct((rows, half), BF),
            jax.ShapeDtypeStruct(old_state.shape, F32),
        ),
        in_specs=[vmem, vmem, anywhere],
        out_specs=(anywhere, anywhere),
        scratch_shapes=[
            pltpu.VMEM((1, width), F32),
            pltpu.VMEM((rows, width), F32),
            pltpu.VMEM((rows, half), BF),
            pltpu.SemaphoreType.DMA((6,)),
        ],
    )(
        pltpu.with_memory_space_constraint(total, pltpu.VMEM),
        pltpu.with_memory_space_constraint(new_state, pltpu.VMEM),
        moe_gain.reshape(1, width),
    )


def solution(mesh):
    in_specs = (
        P("ep", None),
        P("ep", "tp", None),
        P(None, "tp"),
        P(None, "tp"),
        P(None, "tp"),
        P(None, "tp"),
        P("tp"),
        P(),
        P("tp", None),
        P(),
        P("ep", None, "tp"),
        P("ep", None, "tp"),
        P("ep", "tp", None),
        P("ep", None),
        P("ep", None),
        P(),
    )
    out_specs = (P("ep", "tp"), P("ep", "tp", None))
    return jax.shard_map(
        per_device, mesh=mesh, in_specs=in_specs, out_specs=out_specs, check_vma=False
    )
```
